256 devices in a mesh: rep: 64 (over z, y, x_hi), fs: 2 (over core), tp: 2 (over x_lo).
Axes of the slice: x: 4 (x_hi: 2, x_lo: 2; x = x_hi * 2 + x_lo), y: 4, z: 8, core: 2. Of those that a mesh axis runs over, the one named last changes fastest.
Arguments:
- inputs: bfloat16 [16384, 2048], P(('rep', 'fs'), 'tp'), may hold values from -24 to 24
- cotangent: bfloat16 [16384, 2048], P(('rep', 'fs'), 'tp'), may hold values from -24 to 24
- w_up: bfloat16 [2048, 4096], P('fs', 'tp'), may hold values from -0.125 to 0.125
- w_down: bfloat16 [4096, 2048], P('tp', 'fs'), may hold values from -0.09375 to 0.09375
Outputs:
- grad_inputs: bfloat16 [16384, 2048], P(('rep', 'fs'), 'tp')
- grad_up: float32 [2048, 4096], P('fs', 'tp')
- grad_down: float32 [4096, 2048], P('tp', 'fs')
The draws below stay inside these ranges and needn't reach their ends.
All inputs are finite; a program needn't handle non-finite values.
Results may differ from the reference program's by a relative error of at most 0.011.
Values may be sent and summed in bfloat16 or wider, within the bound.
A program may use at most 128 MiB of HBM per device.

```python
import jax
import jax.numpy as jnp
from jax import lax

D = 2048
FF = 4096
TOKENS = 16384
N_TP = 2


def raised(entries, key, source, target, parts, factor):
    owner, partner = [(jnp.arange(entries.shape[axis_at]) // (entries.shape[axis_at] // parts)).reshape([-1 if axis == axis_at else 1 for axis in range(entries.ndim)]) for axis_at in (source, target)]
    chosen = jax.random.permutation(key, parts)[partner]
    strong = (owner == chosen) | (owner == (partner + parts // 2) % parts)
    return jnp.where(strong, factor * entries, entries)


def levels(own_key, shape, pieces, low, largest):
    def one(position, shards_of):
        heights = jax.random.uniform(jax.random.fold_in(jax.random.fold_in(own_key, 6), position), (shards_of,), jnp.float32, low / len(pieces), largest / len(pieces))
        return jnp.repeat(jnp.exp(heights), shape[position] // shards_of).reshape((-1,) + (1,) * (len(shape) - position - 1))

    loudness = one(*pieces[0])
    for cut in pieces[1:]:
        loudness = loudness * one(*cut)
    return loudness


def normal_values(rng, shape, width, most, split=(), dtype=jnp.bfloat16):
    entries = jax.random.normal(rng, shape, jnp.float32) * width
    if len(split) > 0:
        entries = levels(rng, shape, split, -0.22, 0.18) * entries
    return jnp.clip(entries, min=-most, max=most).astype(dtype)


def bell_draw_with(rng, extent, deviation, limit, cuts, heavy, dtype=jnp.bfloat16):
    values = deviation * jax.random.normal(rng, extent, jnp.float32)
    if cuts:
        values = values * levels(rng, extent, cuts, -0.22, 0.18)
    return jnp.clip(raised(values, jax.random.fold_in(rng, 3), *heavy), -limit, limit).astype(dtype)


def setup_inputs(seed: int = 0) -> dict:
    arg_keys = jax.random.split(jax.random.key(seed), 5)
    return {
        "inputs": bell_draw_with(arg_keys[0], (TOKENS, D), 1.0, 24.0, ((0, 128), (1, 2)), (0, 1, 128, 5.5)),
        "cotangent": bell_draw_with(arg_keys[1], (TOKENS, D), 1.0, 24.0, ((0, 128), (1, 2)), (0, 1, 128, 5.5)),
        "w_up": normal_values(arg_keys[2], (D, FF), D ** -0.5, 0.125, ((0, 2), (1, 2))),
        "w_down": normal_values(arg_keys[3], (FF, D), FF ** -0.5, 0.09375, ((0, 2), (1, 2))),
    }


def reference(inputs, cotangent, w_up, w_down):
    preact = jnp.dot(inputs, w_up, preferred_element_type=jnp.float32)
    relu_pre = jnp.maximum(preact, 0.0)
    squared = (relu_pre * relu_pre).astype(jnp.bfloat16)
    act_grad = jnp.dot(cotangent, w_down.T, preferred_element_type=jnp.float32)
    pre_grad = (2.0 * relu_pre * act_grad).astype(jnp.bfloat16)
    grad_up = jnp.dot(inputs.T, pre_grad, preferred_element_type=jnp.float32)
    grad_down = jnp.dot(squared.T, cotangent, preferred_element_type=jnp.float32)
    group = w_up.shape[1] // N_TP
    total = jnp.zeros(inputs.shape, jnp.float32)
    for index in range(N_TP):
        partial_value = jnp.dot(pre_grad[:, index * group:(index + 1) * group],
                          w_up[:, index * group:(index + 1) * group].T,
                          preferred_element_type=jnp.float32).astype(jnp.bfloat16)
        partial_value = lax.optimization_barrier(partial_value)
        total = total + partial_value.astype(jnp.float32)
    return total.astype(jnp.bfloat16), grad_up, grad_down
```

```python
import functools

import jax
import jax.numpy as jnp
from jax import lax
from jax.experimental import pallas as pl
from jax.experimental.pallas import tpu as pltpu
from jax.sharding import PartitionSpec as P

MESH = pl.DeviceIdType.MESH
F32, BF16 = jnp.float32, jnp.bfloat16
NZ, NY, NX = 8, 4, 2
RINGS = {"y": NY, "z": NZ}
TOK, HALF, HID = 128, 1024, 2048
CH = 512
NCH = HID // CH
ROWS = 2 * HALF * HID // 128
TILE = 16
LANES = (("y", "z", 1, 19), ("z", "y", -1, 13), ("y", "z", -1, 19), ("z", "y", 1, 13))
PIECES = NY * NZ
RATE, LAG = 44000.0, 2.2


def hops(n, arm):
    return n // 2 if arm == 0 else n // 2 - 1


def planned():
    order, free, pending, joined = [], {}, [], {}
    now = 0.0

    def send(t, link, rows, what):
        start = max(t, free.get(link, 0.0))
        cost = rows * 256 / RATE * (2.0 if link == "x" else 1.0)
        free[link] = start + cost
        pending.append((start + cost + LAG, len(pending), what))

    def link_of(lane, phase, arm):
        first, second, sign, _ = LANES[lane]
        ring = first if phase in ("rs1", "ag1") else second
        way = sign if arm == 0 else -sign
        return (ring, -way if phase in ("rs1", "rs2") else way)

    def size(lane, phase):
        first, second, _, tiles = LANES[lane]
        piece = tiles * TILE
        return piece * RINGS[second] if phase in ("rs1", "ag1") else piece

    def ring_of(lane, phase):
        return RINGS[LANES[lane][0 if phase in ("rs1", "ag1") else 1]]

    def begin(t, lane, phase):
        order.append(("begin", lane, phase))
        if phase == "x":
            send(t, "x", size(lane, phase), (lane, "x", 0, 1))
            return
        joined[lane, phase] = 0
        for arm in (0, 1):
            send(t, link_of(lane, phase, arm), size(lane, phase), (lane, phase, arm, 1))

    for lane in range(len(LANES)):
        begin(now, lane, "rs1")
    after = {"rs1": "rs2", "rs2": "x", "x": "ag2", "ag2": "ag1", "ag1": None}
    while pending:
        pending.sort()
        at, _, (lane, phase, arm, k) = pending.pop(0)
        now = max(now, at) + 0.1
        last = phase == "x" or k == hops(ring_of(lane, phase), arm)
        if not last:
            order.append(("pass", lane, phase, arm, k))
            send(now, link_of(lane, phase, arm), size(lane, phase), (lane, phase, arm, k + 1))
            continue
        if phase != "x":
            joined[lane, phase] += 1
            if joined[lane, phase] < 2:
                continue
        order.append(("end", lane, phase))
        if after[phase]:
            begin(now, lane, after[phase])
    return order, now


ORDER, ESTIMATE = planned()


def transfers():
    table, rows = {}, 0
    for lane, (first, second, _, tiles) in enumerate(LANES):
        piece = tiles * TILE
        for phase, n, m in (("rs1", RINGS[first], piece * RINGS[second]), ("rs2", RINGS[second], piece)):
            for arm in (0, 1):
                for k in range(1, hops(n, arm) + 1):
                    table[lane, phase, arm, k] = (len(table), rows)
                    rows += m
        table[lane, "x", 0, 1] = (len(table), rows)
        rows += piece
        for phase, n in (("ag2", RINGS[second]), ("ag1", RINGS[first])):
            for arm in (0, 1):
                for k in range(1, hops(n, arm) + 1):
                    table[lane, phase, arm, k] = (len(table), None)
    return table, rows


TABLE, LANDING = transfers()


def dot(a, b, dims):
    return lax.dot_general(a, b, (dims, ((), ())), preferred_element_type=F32)


def body(in_ref, cot_ref, up_ref, down_ref, gin_ref, out_ref,
         x, c, xt, up, down, p_own, p_far, a_own, a_out, a_far, pre, sq, g, land, r, r_in,
         local_sem, xs, xr, ds, dr, gs, gr, ss, rs):
    rep, f, t = lax.axis_index("rep"), lax.axis_index("fs"), lax.axis_index("tp")
    xh = lax.rem(rep, NX)
    yz = rep // NX
    pos = {"y": lax.rem(yz, NY), "z": yz // NY}

    def at(ring, step):
        n = RINGS[ring]
        there = dict(pos)
        there[ring] = lax.rem(pos[ring] + step + n, n)
        return ((there["z"] * NY + there["y"]) * NX + xh, f, t)

    core = (rep, 1 - f, t)
    xpeer = (rep + 1 - 2 * xh, f, t)

    w_copies = [pltpu.make_async_copy(up_ref, up, local_sem.at[0]),
                pltpu.make_async_copy(down_ref, down, local_sem.at[1])]
    for w in w_copies:
        w.start()

    barrier = pltpu.get_barrier_semaphore()
    partners = [core, (rep, 0, 1 - t), (rep, 1, 1 - t), xpeer,
                at("y", 1), at("y", -1), at("z", 1), at("z", -1)]
    for who in partners:
        pl.semaphore_signal(barrier, inc=1, device_id=who, device_id_type=MESH)
    pl.semaphore_wait(barrier, len(partners))

    def remote(src, dst, send, recv, who):
        return pltpu.make_async_remote_copy(
            src_ref=src, dst_ref=dst, send_sem=send, recv_sem=recv, device_id=who, device_id_type=MESH)

    mine = pl.ds(pl.multiple_of(f * TOK, TOK), TOK)
    other = pl.ds(pl.multiple_of((1 - f) * TOK, TOK), TOK)
    home = f == t

    def across(i, src, dst):
        return remote(src, dst.at[mine], xs.at[i], xr.at[i, f], (rep, t, 1 - t))

    def beside(i, src, dst):
        return remote(src, dst.at[mine], xs.at[2 + i], xr.at[i, f], core)

    pairs = ((in_ref, x), (cot_ref, c))
    for i, (src, dst) in enumerate(pairs):
        across(i, src, dst).start()

        @pl.when(home)
        def _():
            dst[mine, :] = src[...]

        @pl.when(jnp.logical_not(home))
        def _():
            beside(i, src, dst).start()

    def landed(i, dst):
        @pl.when(jnp.logical_not(home))
        def _():
            remote(dst.at[mine], dst.at[mine], xs.at[i], xr.at[i, f], core).wait_recv()

        remote(dst.at[other], dst.at[other], xs.at[i], xr.at[i, 1 - f], core).wait_recv()

    def swap_p(i):
        return remote(p_own.at[i], p_far.at[i], ds.at[i], dr.at[i], core)

    def swap_a(i):
        return remote(a_out.at[i], a_far.at[i], ds.at[NCH + i], dr.at[NCH + i], core)

    landed(0, x)
    w_copies[0].wait()
    for i in range(NCH):
        p_own[i] = dot(x[...], up[:, i * CH:(i + 1) * CH], ((1,), (0,)))
        swap_p(i).start()
    xt[...] = x[...].T
    landed(1, c)
    w_copies[1].wait()
    for i in range(NCH):
        part = dot(c[...], down[i * CH:(i + 1) * CH, :], ((1,), (1,)))
        a_own[i] = part
        a_out[i] = part.astype(BF16)
        swap_a(i).start()
    for i in range(NCH):
        swap_p(i).wait_recv()
        swap_a(i).wait_recv()
        relu = jnp.maximum(p_own[i] + p_far[i], 0.0)
        sq[:, i * CH:(i + 1) * CH] = (relu * relu).astype(BF16)
        grad = a_own[i] + a_far[i].astype(F32)
        pre[:, i * CH:(i + 1) * CH] = (2.0 * relu * grad).astype(BF16)

    @pl.loop(0, NCH)
    def _(i):
        cols = pl.ds(pl.multiple_of(i * CH, CH), CH)
        part = dot(xt[...], pre[:, cols], ((1,), (0,)))
        for j in range(CH // 128):
            g[pl.ds(pl.multiple_of((i * (CH // 128) + j) * HALF, HALF), HALF), :] = (
                part[:, j * 128:(j + 1) * 128].astype(BF16))

    @pl.loop(0, NCH)
    def _(i):
        cols = pl.ds(pl.multiple_of(i * CH, CH), CH)
        part = dot(sq[:, cols].T, c[...], ((1,), (0,)))
        for j in range(HALF // 128):
            g[pl.ds(pl.multiple_of(ROWS // 2 + j * HID + i * CH, CH), CH), :] = (
                part[:, j * 128:(j + 1) * 128].astype(BF16))

    bases, base = [], 0
    for first, second, _, tiles in LANES:
        bases.append(base)
        base += tiles * TILE * PIECES
    started = {}

    def facts(lane, phase):
        first, second, sign, tiles = LANES[lane]
        piece = tiles * TILE
        whole = piece * RINGS[second]
        if phase in ("rs1", "ag1"):
            return first, sign, bases[lane], whole
        return second, sign, bases[lane] + pos[first] * whole, piece

    def chunk(lane, phase, step):
        ring, sign, start, rows = facts(lane, phase)
        n = RINGS[ring]
        there = lax.rem(pos[ring] + sign * step + n, n)
        return pl.multiple_of(start + there * rows, TILE), rows

    def send(lane, phase, arm, k):
        index, slot = TABLE[lane, phase, arm, k]
        ring, sign, _, rows = facts(lane, phase)
        way = sign if arm == 0 else -sign
        n = RINGS[ring]
        if phase == "x":
            begin, rows = chunk(lane, phase, 0)
            src, dst, who = g.at[pl.ds(begin, rows)], land.at[pl.ds(slot, rows)], xpeer
        elif slot is not None:
            left = hops(n, arm) - k + 1
            begin, rows = chunk(lane, phase, -left if arm == 0 else left)
            src, dst, who = g.at[pl.ds(begin, rows)], land.at[pl.ds(slot, rows)], at(ring, -way)
        else:
            gone = k - 1
            begin, rows = chunk(lane, phase, -gone if arm == 0 else gone)
            src = dst = out_ref.at[pl.ds(begin, rows)]
            who = at(ring, way)
        copy = remote(src, dst, ss.at[index], rs.at[index], who)
        copy.start()
        started[lane, phase, arm, k] = copy

    def add(target, begin, slots, rows, unit):
        @pl.loop(0, rows // unit)
        def _(i):
            here = pl.ds(pl.multiple_of(begin + i * unit, TILE), unit)
            total = g[here, :].astype(F32)
            for slot in slots:
                total += land[pl.ds(pl.multiple_of(slot + i * unit, TILE), unit), :].astype(F32)
            target[here, :] = total.astype(BF16)

    def run(order):
        for step in order:
            kind, lane, phase = step[:3]
            unit = LANES[lane][3] * TILE
            if kind == "begin":
                send(lane, phase, 0, 1)
                if phase != "x":
                    send(lane, phase, 1, 1)
            elif kind == "pass":
                arm, k = step[3:]
                started[lane, phase, arm, k].wait_recv()
                if phase in ("rs1", "rs2"):
                    left = hops(RINGS[facts(lane, phase)[0]], arm) - k
                    begin, rows = chunk(lane, phase, -left if arm == 0 else left)
                    add(g, begin, (TABLE[lane, phase, arm, k][1],), rows, unit)
                send(lane, phase, arm, k + 1)
            else:
                n = RINGS[facts(lane, phase)[0]]
                lasts = [(lane, phase, 0, 1)] if phase == "x" else [
                    (lane, phase, arm, hops(n, arm)) for arm in (0, 1)]
                for which in lasts:
                    started[which].wait_recv()
                slots = [TABLE[which][1] for which in lasts]
                begin, rows = chunk(lane, phase, 0)
                if phase in ("rs1", "rs2"):
                    add(g, begin, slots, rows, unit)
                elif phase == "x":
                    add(out_ref, begin, slots, rows, unit)

    opening = len(LANES)
    run(ORDER[:opening])

    @pl.loop(0, HALF // 256)
    def _(i):
        rows = pl.ds(pl.multiple_of(i * 256, 256), 256)
        r[:, rows] = dot(pre[...], up[rows, :], ((1,), (1,))).astype(BF16)

    def give(which, src, who):
        return remote(src, r_in.at[t], gs.at[which], gr.at[t], who)

    @pl.when(home)
    def _():
        give(1, r.at[other], core).start()
        r_in[t] = r[mine, :]

    @pl.when(jnp.logical_not(home))
    def _():
        give(0, r.at[pl.ds(0, TOK)], (rep, 0, 1 - t)).start()
        give(1, r.at[pl.ds(TOK, TOK)], (rep, 1, 1 - t)).start()

    half = len(ORDER) // 3
    run(ORDER[opening:half])

    @pl.when(jnp.logical_not(home))
    def _():
        remote(r_in.at[t], r_in.at[t], gs.at[0], gr.at[t], core).wait_recv()

    remote(r_in.at[1 - t], r_in.at[1 - t], gs.at[0], gr.at[1 - t], core).wait_recv()
    gin_ref[...] = (r_in[0].astype(F32) + r_in[1].astype(F32)).astype(BF16)

    run(ORDER[half:])

    for i, (src, dst) in enumerate(pairs):
        across(i, src, dst).wait_send()

        @pl.when(jnp.logical_not(home))
        def _():
            beside(i, src, dst).wait_send()
    for i in range(NCH):
        swap_p(i).wait_send()
        swap_a(i).wait_send()
    give(1, r.at[other], core).wait_send()

    @pl.when(jnp.logical_not(home))
    def _():
        give(0, r.at[other], core).wait_send()
    for copy in started.values():
        copy.wait_send()


def widen(g_ref, up_ref, down_ref):
    i = pl.program_id(0)

    @pl.when(i < 4)
    def _():
        for j in range(4):
            up_ref[:, j * 128:(j + 1) * 128] = g_ref[j * HALF:(j + 1) * HALF, :].astype(F32)

    @pl.when(i >= 4)
    def _():
        for j in range(2):
            down_ref[:, j * 128:(j + 1) * 128] = g_ref[j * HID:(j + 1) * HID, :].astype(F32)


def shards(inputs, cotangent, w_up, w_down):
    vmem, anywhere = pl.BlockSpec(memory_space=pltpu.VMEM), pl.BlockSpec(memory_space=pl.ANY)
    dma = pltpu.SemaphoreType.DMA
    grad_inputs, sums = pl.pallas_call(
        body,
        name="ffn_backward",
        out_shape=(jax.ShapeDtypeStruct((TOK, HALF), BF16), jax.ShapeDtypeStruct((ROWS, 128), BF16)),
        in_specs=[vmem, vmem, anywhere, anywhere],
        out_specs=(vmem, vmem),
        scratch_shapes=[
            pltpu.VMEM((2 * TOK, HALF), BF16), pltpu.VMEM((2 * TOK, HALF), BF16),
            pltpu.VMEM((HALF, 2 * TOK), BF16),
            pltpu.VMEM((HALF, HID), BF16), pltpu.VMEM((HID, HALF), BF16),
            pltpu.VMEM((NCH, 2 * TOK, CH), F32), pltpu.VMEM((NCH, 2 * TOK, CH), F32),
            pltpu.VMEM((NCH, 2 * TOK, CH), F32),
            pltpu.VMEM((NCH, 2 * TOK, CH), BF16), pltpu.VMEM((NCH, 2 * TOK, CH), BF16),
            pltpu.VMEM((2 * TOK, HID), BF16), pltpu.VMEM((2 * TOK, HID), BF16),
            pltpu.VMEM((ROWS, 128), BF16), pltpu.VMEM((LANDING, 128), BF16),
            pltpu.VMEM((2 * TOK, HALF), BF16), pltpu.VMEM((2, TOK, HALF), BF16),
            dma((2,)), dma((4,)), dma((2, 2)), dma((2 * NCH,)), dma((2 * NCH,)), dma((2,)), dma((2,)),
            dma((len(TABLE),)), dma((len(TABLE),)),
        ],
        compiler_params=pltpu.CompilerParams(
            collective_id=0, has_side_effects=True, vmem_limit_bytes=60 * 2**20),
    )(inputs, cotangent, w_up, w_down)
    grad_up, grad_down = pl.pallas_call(
        widen,
        name="widen",
        grid=(8,),
        out_shape=(jax.ShapeDtypeStruct((HALF, HID), F32), jax.ShapeDtypeStruct((HID, HALF), F32)),
        in_specs=[pl.BlockSpec((4096, 128), lambda i: (i, 0))],
        out_specs=(pl.BlockSpec((HALF, 512), lambda i: (0, jnp.minimum(i, 3))),
                   pl.BlockSpec((HID, 256), lambda i: (0, jnp.maximum(i - 4, 0)))),
    )(sums)
    return grad_inputs, grad_up, grad_down


def solution(mesh):
    return jax.shard_map(
        shards,
        mesh=mesh,
        in_specs=(P(("rep", "fs"), "tp"), P(("rep", "fs"), "tp"), P("fs", "tp"), P("tp", "fs")),
        out_specs=(P(("rep", "fs"), "tp"), P("fs", "tp"), P("tp", "fs")),
        check_vma=False,
    )
```

```python
import functools

import jax
import jax.numpy as jnp
from jax import lax
from jax.experimental import pallas as pl
from jax.experimental.pallas import tpu as pltpu
from jax.sharding import PartitionSpec as P

MESH = pl.DeviceIdType.MESH
F32, BF16 = jnp.float32, jnp.bfloat16
NZ, NY, NX = 8, 4, 2
RINGS = {"y": NY, "z": NZ}
TOK, HALF, HID = 128, 1024, 2048
QUARTER = HID // 2
GRP = 2 * TOK
CH = 512
NCH = QUARTER // CH
ROWS = 2 * HALF * QUARTER // 128
TILE = 16
LANES = (("y", "z", 1, 5), ("z", "y", -1, 3), ("y", "z", -1, 5), ("z", "y", 1, 3)) * 2
STARTS = (0.0, 0.0, 1.0, 1.0, 2.5, 2.5, 3.5, 3.5)
PIECES = NY * NZ
RATE, LAG, WINDOW, WORK = 46000.0, 2.0, 3.0, 0.12
DEPTH = {"x": 0, "rs1": 1, "rs2": 1, "ag2": 2, "far2": 2, "ag1": 3, "far1": 3}
FIRST = ("rs1", "ag1", "far1")


def hops(n, arm):
    return n // 2 if arm == 0 else n // 2 - 1


def ring_of(lane, phase):
    return LANES[lane][0 if phase in FIRST else 1]


def length(lane, phase):
    piece = LANES[lane][3] * TILE
    return piece * RINGS[LANES[lane][1]] if phase in FIRST else piece


def last(lane, phase, arm, k):
    return phase == "x" or k == hops(RINGS[ring_of(lane, phase)], arm)


def planned():
    order, free, ready, flying, joined, now = [], {}, [], [], {}, 0.0

    def link_of(lane, phase, arm):
        if phase == "x":
            return "x"
        way = LANES[lane][2] if arm == 0 else -LANES[lane][2]
        return ring_of(lane, phase), -way if phase[:2] == "rs" else way

    def want(lane, phase, arm, k):
        rank = (DEPTH[phase], lane // 2, -k, len(order), len(ready))
        ready.append((rank, link_of(lane, phase, arm), (lane, phase, arm, k)))

    def begin(lane, phase):
        joined[lane, phase] = 0
        for arm in (0,) if phase == "x" else (0, 1):
            want(lane, phase, arm, 1)

    def issue():
        for item in sorted(ready):
            _, link, what = item
            start = max(now, free.get(link, 0.0))
            if start - now < WINDOW:
                ready.remove(item)
                cost = length(what[0], what[1]) * 256 / RATE * (2.0 if link == "x" else 1.0)
                free[link] = start + cost
                flying.append((start + cost + LAG, len(order), what))
                order.append(("send",) + what)

    todo = sorted((at, lane) for lane, at in enumerate(STARTS))
    while todo or flying:
        flying.sort()
        if todo and (not flying or todo[0][0] <= flying[0][0]):
            at, lane = todo.pop(0)
            now = max(now, at)
            order.append(("begin", lane))
            begin(lane, "rs1")
        else:
            at, _, (lane, phase, arm, k) = flying.pop(0)
            now = max(now, at) + WORK
            if not last(lane, phase, arm, k):
                order.append(("pass", lane, phase, arm, k))
                want(lane, phase, arm, k + 1)
            else:
                joined[lane, phase] += 1
                if phase == "x" or joined[lane, phase] == 2:
                    order.append(("end", lane, phase))
                    for after in {"rs1": ("rs2",), "rs2": ("x", "ag2"), "x": ("far2",),
                                  "ag2": ("ag1",), "far2": ("far1",)}.get(phase, ()):
                        begin(lane, after)
        issue()
        if ready and not flying and not todo:
            now = min(free[link] for _, link, _ in ready)
            issue()
    return order, now


ORDER, ESTIMATE = planned()


def transfers():
    table, rows = {}, 0
    for lane in range(len(LANES)):
        for phase in ("rs1", "rs2", "x", "ag2", "ag1", "far2", "far1"):
            for arm in (0,) if phase == "x" else (0, 1):
                for k in range(1, 2 if phase == "x" else hops(RINGS[ring_of(lane, phase)], arm) + 1):
                    lands = phase[:2] == "rs"
                    table[lane, phase, arm, k] = (len(table), rows if lands else None)
                    rows += length(lane, phase) if lands else 0
    return table, rows


TABLE, LANDING = transfers()


def dot(a, b, dims):
    return lax.dot_general(a, b, (dims, ((), ())), preferred_element_type=F32)


def body(in_ref, cot_ref, up_ref, down_ref, gin_ref, out_ref,
         x, c, xt, sqt, up, down, p_own, p_far, a_own, a_out, a_far, pre, sq, g, land, r, r_in,
         local_sem, xs, xr, fsem, ds, dr, gs, gr, ss, rs):
    rep, f, t = lax.axis_index("rep"), lax.axis_index("fs"), lax.axis_index("tp")
    xh = lax.rem(rep, NX)
    yz = rep // NX
    xpos = xh * 2 + t
    pos = {"y": lax.rem(yz, NY), "z": yz // NY}

    def at(ring, step):
        n = RINGS[ring]
        there = dict(pos)
        there[ring] = lax.rem(pos[ring] + step + n, n)
        return ((there["z"] * NY + there["y"]) * NX + xh, f, t)

    def along(step, who):
        there = lax.rem(xpos + step + 4, 4)
        return (yz * NX + there // 2, who, lax.rem(there, 2))

    core = (rep, 1 - f, t)
    xpeer = (yz * NX + 1 - xh, f, t)
    home = f == t
    away = jnp.logical_not(home)

    share = pl.ds(pl.multiple_of(xh * QUARTER, QUARTER), QUARTER)
    w_copies = [pltpu.make_async_copy(up_ref.at[:, share], up, local_sem.at[0]),
                pltpu.make_async_copy(down_ref.at[share, :], down, local_sem.at[1])]
    for w in w_copies:
        w.start()

    barrier = pltpu.get_barrier_semaphore()
    partners = [core] + [along(step, who) for step in (1, -1, 2) for who in (0, 1)] + [
        at("y", 1), at("y", -1), at("z", 1), at("z", -1)]
    for who in partners:
        pl.semaphore_signal(barrier, inc=1, device_id=who, device_id_type=MESH)
    pl.semaphore_wait(barrier, len(partners))

    def remote(src, dst, send, recv, who):
        return pltpu.make_async_remote_copy(
            src_ref=src, dst_ref=dst, send_sem=send, recv_sem=recv, device_id=who, device_id_type=MESH)

    def block(group, who):
        return pl.ds(pl.multiple_of((group * 2 + who) * TOK, TOK), TOK)

    pairs = ((in_ref, x), (cot_ref, c))

    def across(i, way):
        src, dst = pairs[i]
        group = t if way == 1 else 1 - t
        return remote(src, dst.at[block(group, f)], xs.at[i, 0 if way == 1 else 1],
                      xr.at[i, group * 2 + f], along(way, t))

    def beside(i):
        src, dst = pairs[i]
        return remote(src, dst.at[block(0, f)], xs.at[i, 2], xr.at[i, f], core)

    def onward(i, way):
        _, dst = pairs[i]
        group, who = (1 - t, 0) if way == 1 else (t, 1)
        return remote(dst.at[block(group, who)], dst.at[block(1, who)], fsem.at[i, who],
                      xr.at[i, 2 + who], along(way, f))

    def landed(i, group, who):
        _, dst = pairs[i]
        there = dst.at[block(group, who)]
        remote(there, there, xs.at[i, 0], xr.at[i, group * 2 + who], core).wait_recv()

    for i in (0, 1):
        across(i, 1).start()
        across(i, -1).start()
        src, dst = pairs[i]

        @pl.when(home)
        def _():
            dst[block(0, f), :] = src[...]

        @pl.when(away)
        def _():
            beside(i).start()

    def pass_on(i):
        @pl.when(away)
        def _():
            landed(i, 1 - t, 0)
            onward(i, 1).start()
            landed(i, t, 1)
            onward(i, -1).start()

    def arrive(i, group):
        if group == 0:
            @pl.when(home)
            def _():
                landed(i, 0, 1 - f)
        else:
            @pl.when(home)
            def _():
                landed(i, 1, 0)
                landed(i, 1, 1)

        @pl.when(away)
        def _():
            landed(i, group, jnp.where(group == t, 0, 1))

    def swap_p(i):
        return remote(p_own.at[i], p_far.at[i], ds.at[i], dr.at[i], core)

    def swap_a(i):
        return remote(a_out.at[i], a_far.at[i], ds.at[2 * NCH + i], dr.at[2 * NCH + i], core)

    def first_product(group):
        arrive(0, group)
        here = pl.ds(group * GRP, GRP)
        for j in range(NCH):
            i = group * NCH + j
            p_own[i] = dot(x[here, :], up[:, j * CH:(j + 1) * CH], ((1,), (0,)))
            swap_p(i).start()
        xt[:, here] = x[here, :].T

    def second_product(group):
        arrive(1, group)
        here = pl.ds(group * GRP, GRP)
        for j in range(NCH):
            i = group * NCH + j
            part = dot(c[here, :], down[j * CH:(j + 1) * CH, :], ((1,), (1,)))
            a_own[i] = part
            a_out[i] = part.astype(BF16)
            swap_a(i).start()

    pass_on(0)
    for w in w_copies:
        w.wait()
    first_product(0)
    pass_on(1)
    second_product(0)
    first_product(1)
    second_product(1)

    def activations(j):
        cols = slice(j * CH, (j + 1) * CH)
        for group in (0, 1):
            i = group * NCH + j
            swap_p(i).wait_recv()
            swap_a(i).wait_recv()
            here = slice(group * GRP, (group + 1) * GRP)
            relu = jnp.maximum(p_own[i] + p_far[i], 0.0)
            sq[here, cols] = (relu * relu).astype(BF16)
            grad = a_own[i] + a_far[i].astype(F32)
            pre[here, cols] = (2.0 * relu * grad).astype(BF16)

    def local_up(j):
        activations(j)
        part = dot(xt[...], pre[:, j * CH:(j + 1) * CH], ((1,), (0,)))
        for k in range(CH // 128):
            g[(j * 4 + k) * HALF:(j * 4 + k + 1) * HALF, :] = part[:, k * 128:(k + 1) * 128].astype(BF16)

    def local_down(j):
        if j == 0:
            sqt[...] = sq[...].T
        part = dot(sqt[...], c[:, j * CH:(j + 1) * CH], ((1,), (0,)))
        for k in range(CH // 128):
            g[(8 + j * 4 + k) * HALF:(9 + j * 4 + k) * HALF, :] = part[:, k * 128:(k + 1) * 128].astype(BF16)

    def inputs_part(j):
        rows = slice(j * 256, (j + 1) * 256)
        r[:, rows] = dot(pre[...], up[rows, :], ((1,), (1,))).astype(BF16)

    def give(group, who):
        there = jnp.where(group == 0, xh, 1 - xh)
        return remote(r.at[block(group, who)], r_in.at[xpos], gs.at[group, who], gr.at[xpos],
                      (yz * NX + there, who, f))

    def give_all():
        @pl.when(home)
        def _():
            give(0, 1 - f).start()
            r_in[xpos] = r[block(0, f), :]

        @pl.when(away)
        def _():
            give(0, f).start()
            give(0, 1 - f).start()

        give(1, 0).start()
        give(1, 1).start()

    def inputs_sum():
        def came(k):
            there = r_in.at[k]
            remote(there, there, gs.at[0, 0], gr.at[k], core).wait_recv()

        @pl.when(away)
        def _():
            came(xpos)

        for step in (1, 2, 3):
            came(lax.rem(xpos + step, 4))
        total = r_in[0].astype(F32)
        for k in range(1, 4):
            total += r_in[k].astype(F32)
        gin_ref[...] = total.astype(BF16)

    bases, base = [], 0
    for lane in range(len(LANES)):
        bases.append(base)
        base += LANES[lane][3] * TILE * PIECES
    started = {}

    def chunk(lane, phase, step):
        ring = ring_of(lane, phase)
        rows = length(lane, phase)
        start = bases[lane]
        if phase not in FIRST:
            start += pos[LANES[lane][0]] * length(lane, "rs1")
        if phase[:2] == "ag" or phase == "x":
            start += xh * ROWS
        elif phase[:3] == "far":
            start += (1 - xh) * ROWS
        n = RINGS[ring]
        there = lax.rem(pos[ring] + LANES[lane][2] * step + n, n)
        return pl.multiple_of(start + there * rows, TILE), rows

    def send(lane, phase, arm, k):
        index, slot = TABLE[lane, phase, arm, k]
        ring = ring_of(lane, phase)
        way = LANES[lane][2] if arm == 0 else -LANES[lane][2]
        if phase == "x":
            begin, rows = chunk(lane, phase, 0)
            src = dst = out_ref.at[pl.ds(begin, rows)]
            who = xpeer
        elif slot is not None:
            left = hops(RINGS[ring], arm) - k + 1
            begin, rows = chunk(lane, phase, -left if arm == 0 else left)
            src, dst, who = g.at[pl.ds(begin, rows)], land.at[pl.ds(slot, rows)], at(ring, -way)
        else:
            begin, rows = chunk(lane, phase, 1 - k if arm == 0 else k - 1)
            src = dst = out_ref.at[pl.ds(begin, rows)]
            who = at(ring, way)
        copy = remote(src, dst, ss.at[index], rs.at[index], who)
        copy.start()
        started[lane, phase, arm, k] = copy

    def add(target, shift, begin, slots, rows, unit):
        @pl.loop(0, rows // unit)
        def _(i):
            here = pl.multiple_of(begin + i * unit, TILE)
            total = g[pl.ds(here, unit), :].astype(F32)
            for slot in slots:
                total += land[pl.ds(pl.multiple_of(slot + i * unit, TILE), unit), :].astype(F32)
            target[pl.ds(pl.multiple_of(here + shift, TILE), unit), :] = total.astype(BF16)

    aside = [functools.partial(inputs_part, j) for j in range(4)] + [give_all]
    begun = 0
    for count, step in enumerate(ORDER):
        kind, lane = step[:2]
        unit = LANES[lane][3] * TILE
        if kind == "begin":
            begun += 1
            if lane % 2 == 0:
                (local_up, local_down)[lane // 4](lane // 2 % 2)
        elif kind == "send":
            send(*step[1:])
        elif kind == "pass":
            phase, arm, k = step[2:]
            started[lane, phase, arm, k].wait_recv()
            if phase[:2] == "rs":
                left = hops(RINGS[ring_of(lane, phase)], arm) - k
                begin, rows = chunk(lane, phase, -left if arm == 0 else left)
                add(g, 0, begin, (TABLE[lane, phase, arm, k][1],), rows, unit)
            if begun == len(LANES) and aside:
                aside.pop(0)()
        else:
            phase = step[2]
            n = RINGS[ring_of(lane, phase)]
            ends = [(lane, phase, 0, 1)] if phase == "x" else [
                (lane, phase, arm, hops(n, arm)) for arm in (0, 1)]
            for which in ends:
                started[which].wait_recv()
            if phase[:2] == "rs":
                begin, rows = chunk(lane, phase, 0)
                into, shift = (g, 0) if phase == "rs1" else (out_ref, xh * ROWS)
                add(into, shift, begin, [TABLE[which][1] for which in ends], rows, unit)
        if count == len(ORDER) * 3 // 5:
            inputs_sum()

    for i in (0, 1):
        across(i, 1).wait_send()
        across(i, -1).wait_send()

        @pl.when(away)
        def _():
            beside(i).wait_send()
            onward(i, 1).wait_send()
            onward(i, -1).wait_send()
    for i in range(2 * NCH):
        swap_p(i).wait_send()
        swap_a(i).wait_send()

    give(0, 1 - f).wait_send()
    give(1, 0).wait_send()
    give(1, 1).wait_send()

    @pl.when(away)
    def _():
        give(0, f).wait_send()
    for copy in started.values():
        copy.wait_send()


def widen(g_ref, up_ref, down_ref):
    i = lax.rem(pl.program_id(0), 4)

    @pl.when(i < 2)
    def _():
        for j in range(4):
            up_ref[:, j * 128:(j + 1) * 128] = g_ref[j * HALF:(j + 1) * HALF, :].astype(F32)

    @pl.when(i >= 2)
    def _():
        for j in range(4):
            down_ref[:, j * 128:(j + 1) * 128] = g_ref[j * HALF:(j + 1) * HALF, :].astype(F32)


def shards(inputs, cotangent, w_up, w_down):
    vmem, anywhere = pl.BlockSpec(memory_space=pltpu.VMEM), pl.BlockSpec(memory_space=pl.ANY)
    dma = pltpu.SemaphoreType.DMA
    grad_inputs, sums = pl.pallas_call(
        body,
        name="ffn_backward",
        out_shape=(jax.ShapeDtypeStruct((TOK, HALF), BF16), jax.ShapeDtypeStruct((2 * ROWS, 128), BF16)),
        in_specs=[vmem, vmem, anywhere, anywhere],
        out_specs=(vmem, vmem),
        scratch_shapes=[
            pltpu.VMEM((2 * GRP, HALF), BF16), pltpu.VMEM((2 * GRP, HALF), BF16),
            pltpu.VMEM((HALF, 2 * GRP), BF16), pltpu.VMEM((QUARTER, 2 * GRP), BF16),
            pltpu.VMEM((HALF, QUARTER), BF16), pltpu.VMEM((QUARTER, HALF), BF16),
            pltpu.VMEM((2 * NCH, GRP, CH), F32), pltpu.VMEM((2 * NCH, GRP, CH), F32),
            pltpu.VMEM((2 * NCH, GRP, CH), F32),
            pltpu.VMEM((2 * NCH, GRP, CH), BF16), pltpu.VMEM((2 * NCH, GRP, CH), BF16),
            pltpu.VMEM((2 * GRP, QUARTER), BF16), pltpu.VMEM((2 * GRP, QUARTER), BF16),
            pltpu.VMEM((ROWS, 128), BF16), pltpu.VMEM((LANDING, 128), BF16),
            pltpu.VMEM((2 * GRP, HALF), BF16), pltpu.VMEM((4, TOK, HALF), BF16),
            dma((2,)), dma((2, 3)), dma((2, 4)), dma((2, 2)), dma((4 * NCH,)), dma((4 * NCH,)),
            dma((2, 2)), dma((4,)), dma((len(TABLE),)), dma((len(TABLE),)),
        ],
        compiler_params=pltpu.CompilerParams(
            collective_id=0, has_side_effects=True, vmem_limit_bytes=60 * 2**20),
    )(inputs, cotangent, w_up, w_down)
    grad_up, grad_down = pl.pallas_call(
        widen,
        name="widen",
        grid=(8,),
        out_shape=(jax.ShapeDtypeStruct((HALF, HID), F32), jax.ShapeDtypeStruct((HID, HALF), F32)),
        in_specs=[pl.BlockSpec((4096, 128), lambda i: (i, 0))],
        out_specs=(
            pl.BlockSpec((HALF, 512), lambda i: (0, i // 4 * 2 + jnp.minimum(lax.rem(i, 4), 1))),
            pl.BlockSpec((HALF, 512), lambda i: (i // 4, jnp.maximum(lax.rem(i, 4) - 2, 0)))),
    )(sums)
    return grad_inputs, grad_up, grad_down


def solution(mesh):
    return jax.shard_map(
        shards,
        mesh=mesh,
        in_specs=(P(("rep", "fs"), "tp"), P(("rep", "fs"), "tp"), P("fs", "tp"), P("tp", "fs")),
        out_specs=(P(("rep", "fs"), "tp"), P("fs", "tp"), P("tp", "fs")),
        check_vma=False,
    )
```

```python
import functools
import heapq

import jax
import jax.numpy as jnp
from jax import lax
from jax.experimental import pallas as pl
from jax.experimental.pallas import tpu as pltpu
from jax.sharding import PartitionSpec as P

MESH = pl.DeviceIdType.MESH
F32, BF16 = jnp.float32, jnp.bfloat16
NZ, NY, NX = 8, 4, 2
RINGS = {"y": NY, "z": NZ}
TOK, HALF, HID = 128, 1024, 2048
QUARTER = HID // 2
GRP = 2 * TOK
CH = 512
NCH = QUARTER // CH
ROWS = 2 * HALF * QUARTER // 128
TILE = 16
A, B = ("y", "z"), ("z", "y")
LANES = ((*A, 1, 3), (*B, -1, 2), (*A, -1, 3), (*B, 1, 2), (*A, 1, 3), (*B, -1, 2), (*A, -1, 3),
         (*A, 1, 3), (*B, 1, 2), (*A, -1, 3), (*B, -1, 2), (*A, 1, 1), (*B, 1, 2), (*A, -1, 1))
UPTO = tuple(sum(lane[3] for lane in LANES[:i + 1]) for i in range(len(LANES)))
STARTS = tuple(2.4 * tiles / 32 for tiles in UPTO)
PIECES = NY * NZ
RATE, LAG, WINDOW, WORK = 46000.0, 2.0, 1.6, 0.12
RANKS = {
    "rs1": (8, 39, 32, 19, 44, 56, 71, 34, 12, 58, 65, 47, 29, 68),
    "rs2": (16, 70, 64, 91, 37, 17, 83, 21, 78, 72, 95, 84, 80, 87),
    "x": (46, 59, 52, 74, 51, 3, 48, 0, 61, 50, 18, 88, 41, 9),
    "ag2": (35, 24, 40, 62, 13, 94, 77, 55, 57, 67, 85, 66, 27, 43),
    "ag1": (42, 97, 75, 38, 10, 14, 11, 2, 81, 86, 54, 53, 79, 45),
    "far2": (4, 33, 22, 23, 31, 30, 73, 63, 82, 5, 49, 69, 28, 60),
    "far1": (15, 89, 1, 76, 25, 90, 92, 7, 96, 26, 6, 36, 20, 93)}
FIRST = ("rs1", "ag1", "far1")


def hops(n, arm):
    return n // 2 if arm == 0 else n // 2 - 1


def ring_of(lane, phase):
    return LANES[lane][0 if phase in FIRST else 1]


def length(lane, phase):
    piece = LANES[lane][3] * TILE
    return piece * RINGS[LANES[lane][1]] if phase in FIRST else piece


def last(lane, phase, arm, k):
    return phase == "x" or k == hops(RINGS[ring_of(lane, phase)], arm)


def planned():
    order, free, ready, flying, joined, now, count = [], {}, {}, [], {}, 0.0, 0

    def link_of(lane, phase, arm):
        if phase == "x":
            return "x"
        way = LANES[lane][2] if arm == 0 else -LANES[lane][2]
        return ring_of(lane, phase), -way if phase[:2] == "rs" else way

    def want(lane, phase, arm, k):
        nonlocal count
        count += 1
        line = ready.setdefault(link_of(lane, phase, arm), [])
        heapq.heappush(line, (RANKS[phase][lane], -k, count, (lane, phase, arm, k)))

    def begin(lane, phase):
        joined[lane, phase] = 0
        for arm in (0,) if phase == "x" else (0, 1):
            want(lane, phase, arm, 1)

    def issue():
        nonlocal count
        for link, line in ready.items():
            while line and max(now, free.get(link, 0.0)) - now < WINDOW:
                what = heapq.heappop(line)[3]
                cost = length(what[0], what[1]) * 256 * (2 if link == "x" else 1) / RATE
                free[link] = max(now, free.get(link, 0.0)) + cost
                count += 1
                heapq.heappush(flying, (free[link] + LAG, count, what))
                order.append(("send",) + what)

    todo = sorted((at, lane) for lane, at in enumerate(STARTS))
    while todo or flying:
        if todo and (not flying or todo[0][0] <= flying[0][0]):
            at, lane = todo.pop(0)
            now = max(now, at)
            order.append(("begin", lane))
            begin(lane, "rs1")
        else:
            at, _, (lane, phase, arm, k) = heapq.heappop(flying)
            now = max(now, at) + WORK
            if not last(lane, phase, arm, k):
                order.append(("pass", lane, phase, arm, k))
                want(lane, phase, arm, k + 1)
            else:
                joined[lane, phase] += 1
                if phase == "x" or joined[lane, phase] == 2:
                    order.append(("end", lane, phase))
                    for after in {"rs1": ("rs2",), "rs2": ("x", "ag2"), "x": ("far2",),
                                  "ag2": ("ag1",), "far2": ("far1",)}.get(phase, ()):
                        begin(lane, after)
        issue()
        if not flying and not todo and any(ready.values()):
            now = min(free[link] for link, line in ready.items() if line)
            issue()
    return order, now


ORDER, ESTIMATE = planned()


def transfers():
    table, rows = {}, 0
    for lane in range(len(LANES)):
        for phase in ("rs1", "rs2", "x", "ag2", "ag1", "far2", "far1"):
            for arm in (0,) if phase == "x" else (0, 1):
                for k in range(1, 2 if phase == "x" else hops(RINGS[ring_of(lane, phase)], arm) + 1):
                    lands = phase[:2] == "rs"
                    table[lane, phase, arm, k] = (len(table), rows if lands else None)
                    rows += length(lane, phase) if lands else 0
    return table, rows


TABLE, LANDING = transfers()


def dot(a, b, dims):
    return lax.dot_general(a, b, (dims, ((), ())), preferred_element_type=F32)


def body(in_ref, cot_ref, up_ref, down_ref, gin_ref, sums_ref,
         in_v, cot_v, out_ref, x, c, xt, sqt, up, down, p_own, p_far, a_own, a_out, a_far, pre, sq, g, land, r, r_in,
         local_sem, xs, xr, fsem, ds, dr, gs, gr, ss, rs, os):
    rep, f, t = lax.axis_index("rep"), lax.axis_index("fs"), lax.axis_index("tp")
    xh = lax.rem(rep, NX)
    yz = rep // NX
    xpos = xh * 2 + t
    pos = {"y": lax.rem(yz, NY), "z": yz // NY}

    def at(ring, step):
        n = RINGS[ring]
        there = dict(pos)
        there[ring] = lax.rem(pos[ring] + step + n, n)
        return ((there["z"] * NY + there["y"]) * NX + xh, f, t)

    def along(step, who):
        there = lax.rem(xpos + step + 4, 4)
        return (yz * NX + there // 2, who, lax.rem(there, 2))

    core = (rep, 1 - f, t)
    xpeer = (yz * NX + 1 - xh, f, t)
    home = f == t
    away = jnp.logical_not(home)

    share = pl.ds(pl.multiple_of(xh * QUARTER, QUARTER), QUARTER)
    w_copies = [pltpu.make_async_copy(up_ref.at[:, share], up, local_sem.at[0]),
                pltpu.make_async_copy(down_ref.at[share, :], down, local_sem.at[1])]
    t_copies = [pltpu.make_async_copy(in_ref, in_v, local_sem.at[2]),
                pltpu.make_async_copy(cot_ref, cot_v, local_sem.at[3])]
    for copy in t_copies + w_copies:
        copy.start()

    barrier = pltpu.get_barrier_semaphore()
    partners = [core] + [along(step, who) for step in (1, -1, 2) for who in (0, 1)] + [
        at("y", 1), at("y", -1), at("z", 1), at("z", -1)]
    for who in partners:
        pl.semaphore_signal(barrier, inc=1, device_id=who, device_id_type=MESH)
    pl.semaphore_wait(barrier, len(partners))

    def remote(src, dst, send, recv, who):
        return pltpu.make_async_remote_copy(
            src_ref=src, dst_ref=dst, send_sem=send, recv_sem=recv, device_id=who, device_id_type=MESH)

    def block(group, who):
        return pl.ds(pl.multiple_of((group * 2 + who) * TOK, TOK), TOK)

    pairs = ((in_v, x), (cot_v, c))

    def across(i, way):
        src, dst = pairs[i]
        group = t if way == 1 else 1 - t
        return remote(src, dst.at[block(group, f)], xs.at[i, 0 if way == 1 else 1],
                      xr.at[i, group * 2 + f], along(way, t))

    def beside(i):
        src, dst = pairs[i]
        return remote(src, dst.at[block(0, f)], xs.at[i, 2], xr.at[i, f], core)

    def onward(i, way):
        _, dst = pairs[i]
        group, who = (1 - t, 0) if way == 1 else (t, 1)
        return remote(dst.at[block(group, who)], dst.at[block(1, who)], fsem.at[i, who],
                      xr.at[i, 2 + who], along(way, f))

    def landed(i, group, who):
        _, dst = pairs[i]
        there = dst.at[block(group, who)]
        remote(there, there, xs.at[i, 0], xr.at[i, group * 2 + who], core).wait_recv()

    for i in (0, 1):
        t_copies[i].wait()
        across(i, 1).start()
        across(i, -1).start()
        src, dst = pairs[i]

        @pl.when(home)
        def _():
            dst[block(0, f), :] = src[...]

        @pl.when(away)
        def _():
            beside(i).start()

    def pass_on(i):
        @pl.when(away)
        def _():
            landed(i, 1 - t, 0)
            onward(i, 1).start()
            landed(i, t, 1)
            onward(i, -1).start()

    def arrive(i, group):
        if group == 0:
            @pl.when(home)
            def _():
                landed(i, 0, 1 - f)
        else:
            @pl.when(home)
            def _():
                landed(i, 1, 0)
                landed(i, 1, 1)

        @pl.when(away)
        def _():
            landed(i, group, jnp.where(group == t, 0, 1))

    def swap_p(i):
        return remote(p_own.at[i], p_far.at[i], ds.at[i], dr.at[i], core)

    def swap_a(i):
        return remote(a_out.at[i], a_far.at[i], ds.at[2 * NCH + i], dr.at[2 * NCH + i], core)

    def first_product(group):
        arrive(0, group)
        here = pl.ds(group * GRP, GRP)
        for j in range(NCH):
            i = group * NCH + j
            p_own[i] = dot(x[here, :], up[:, j * CH:(j + 1) * CH], ((1,), (0,)))
            swap_p(i).start()
        xt[:, here] = x[here, :].T

    def second_product(group):
        arrive(1, group)
        here = pl.ds(group * GRP, GRP)
        for j in range(NCH):
            i = group * NCH + j
            part = dot(c[here, :], down[j * CH:(j + 1) * CH, :], ((1,), (1,)))
            a_own[i] = part
            a_out[i] = part.astype(BF16)
            swap_a(i).start()

    pass_on(0)
    for w in w_copies:
        w.wait()
    first_product(0)
    pass_on(1)
    second_product(0)
    first_product(1)
    second_product(1)

    def activations(j):
        cols = slice(j * CH, (j + 1) * CH)
        for group in (0, 1):
            i = group * NCH + j
            swap_p(i).wait_recv()
            swap_a(i).wait_recv()
            here = slice(group * GRP, (group + 1) * GRP)
            relu = jnp.maximum(p_own[i] + p_far[i], 0.0)
            sq[here, cols] = (relu * relu).astype(BF16)
            grad = a_own[i] + a_far[i].astype(F32)
            pre[here, cols] = (2.0 * relu * grad).astype(BF16)

    def local_up(j):
        activations(j)
        part = dot(xt[...], pre[:, j * CH:(j + 1) * CH], ((1,), (0,)))
        for k in range(CH // 128):
            g[(j * 4 + k) * HALF:(j * 4 + k + 1) * HALF, :] = part[:, k * 128:(k + 1) * 128].astype(BF16)

    def local_down(j):
        if j == 0:
            sqt[...] = sq[...].T
        part = dot(sqt[...], c[:, j * CH:(j + 1) * CH], ((1,), (0,)))
        for k in range(CH // 128):
            g[(8 + j * 4 + k) * HALF:(9 + j * 4 + k) * HALF, :] = part[:, k * 128:(k + 1) * 128].astype(BF16)

    def inputs_part(j):
        rows = slice(j * 256, (j + 1) * 256)
        r[:, rows] = dot(pre[...], up[rows, :], ((1,), (1,))).astype(BF16)

    def give(group, who):
        there = jnp.where(group == 0, xh, 1 - xh)
        return remote(r.at[block(group, who)], r_in.at[xpos], gs.at[group, who], gr.at[xpos],
                      (yz * NX + there, who, f))

    def give_all():
        @pl.when(home)
        def _():
            give(0, 1 - f).start()
            r_in[xpos] = r[block(0, f), :]

        @pl.when(away)
        def _():
            give(0, f).start()
            give(0, 1 - f).start()

        give(1, 0).start()
        give(1, 1).start()

    def inputs_sum():
        def came(k):
            there = r_in.at[k]
            remote(there, there, gs.at[0, 0], gr.at[k], core).wait_recv()

        @pl.when(away)
        def _():
            came(xpos)

        for step in (1, 2, 3):
            came(lax.rem(xpos + step, 4))
        total = r_in[0].astype(F32)
        for k in range(1, 4):
            total += r_in[k].astype(F32)
        gin_ref[...] = total.astype(BF16)

    bases, base = [], 0
    for lane in range(len(LANES)):
        bases.append(base)
        base += LANES[lane][3] * TILE * PIECES
    started = {}

    def chunk(lane, phase, step):
        ring = ring_of(lane, phase)
        rows = length(lane, phase)
        start = bases[lane]
        if phase not in FIRST:
            start += pos[LANES[lane][0]] * length(lane, "rs1")
        if phase[:2] == "ag" or phase == "x":
            start += xh * ROWS
        elif phase[:3] == "far":
            start += (1 - xh) * ROWS
        n = RINGS[ring]
        there = lax.rem(pos[ring] + LANES[lane][2] * step + n, n)
        return pl.multiple_of(start + there * rows, TILE), rows

    def send(lane, phase, arm, k):
        index, slot = TABLE[lane, phase, arm, k]
        ring = ring_of(lane, phase)
        way = LANES[lane][2] if arm == 0 else -LANES[lane][2]
        if phase == "x":
            begin, rows = chunk(lane, phase, 0)
            src = dst = out_ref.at[pl.ds(begin, rows)]
            who = xpeer
        elif slot is not None:
            left = hops(RINGS[ring], arm) - k + 1
            begin, rows = chunk(lane, phase, -left if arm == 0 else left)
            src, dst, who = g.at[pl.ds(begin, rows)], land.at[pl.ds(slot, rows)], at(ring, -way)
        else:
            begin, rows = chunk(lane, phase, 1 - k if arm == 0 else k - 1)
            src = dst = out_ref.at[pl.ds(begin, rows)]
            who = at(ring, way)
        copy = remote(src, dst, ss.at[index], rs.at[index], who)
        copy.start()
        started[lane, phase, arm, k] = copy

    def add(target, shift, begin, slots, rows):
        unit = max(u for u in range(TILE, 193, TILE) if rows % u == 0)

        @pl.loop(0, rows // unit)
        def _(i):
            here = pl.multiple_of(begin + i * unit, TILE)
            total = g[pl.ds(here, unit), :].astype(F32)
            for slot in slots:
                total += land[pl.ds(pl.multiple_of(slot + i * unit, TILE), unit), :].astype(F32)
            target[pl.ds(pl.multiple_of(here + shift, TILE), unit), :] = total.astype(BF16)

    aside = [functools.partial(inputs_part, j) for j in range(4)] + [give_all]
    leaving = []
    begun = chunks = 0
    for count, step in enumerate(ORDER):
        kind, lane = step[:2]
        if kind == "begin":
            begun += 1
            while chunks * 8 < UPTO[lane]:
                (local_up, local_down)[chunks // 2](chunks % 2)
                chunks += 1
        elif kind == "send":
            send(*step[1:])
        elif kind == "pass":
            phase, arm, k = step[2:]
            started[lane, phase, arm, k].wait_recv()
            if phase[:2] == "rs":
                left = hops(RINGS[ring_of(lane, phase)], arm) - k
                begin, rows = chunk(lane, phase, -left if arm == 0 else left)
                add(g, 0, begin, (TABLE[lane, phase, arm, k][1],), rows)
            if begun == len(LANES) and aside:
                aside.pop(0)()
        else:
            phase = step[2]
            n = RINGS[ring_of(lane, phase)]
            ends = [(lane, phase, 0, 1)] if phase == "x" else [
                (lane, phase, arm, hops(n, arm)) for arm in (0, 1)]
            for which in ends:
                started[which].wait_recv()
            if phase[:2] == "rs":
                begin, rows = chunk(lane, phase, 0)
                into, shift = (g, 0) if phase == "rs1" else (out_ref, xh * ROWS)
                add(into, shift, begin, [TABLE[which][1] for which in ends], rows)
            elif phase in ("ag1", "far1"):
                half = xh if phase == "ag1" else 1 - xh
                there = pl.ds(pl.multiple_of(half * ROWS + bases[lane], TILE), LANES[lane][3] * TILE * PIECES)
                leaving.append(pltpu.make_async_copy(
                    out_ref.at[there], sums_ref.at[there], os.at[len(leaving)]))
                leaving[-1].start()
        if count == len(ORDER) * 3 // 5:
            inputs_sum()

    for i in (0, 1):
        across(i, 1).wait_send()
        across(i, -1).wait_send()

        @pl.when(away)
        def _():
            beside(i).wait_send()
            onward(i, 1).wait_send()
            onward(i, -1).wait_send()
    for i in range(2 * NCH):
        swap_p(i).wait_send()
        swap_a(i).wait_send()

    give(0, 1 - f).wait_send()
    give(1, 0).wait_send()
    give(1, 1).wait_send()

    @pl.when(away)
    def _():
        give(0, f).wait_send()
    for copy in started.values():
        copy.wait_send()
    for copy in leaving:
        copy.wait()


PARTS = 8


def widen(gin_ref, sums_ref, gin_out, up_out, down_out, gin, narrow, wide, sem, read, write):
    through = pltpu.make_async_copy(gin_ref, gin, sem.at[0])
    through.start()
    rows, columns = 2 * ROWS // PARTS, 2 * ROWS // PARTS // HALF
    reads = []
    for i in range(PARTS):
        there = pl.ds(i * rows, rows)
        reads.append(pltpu.make_async_copy(sums_ref.at[there], narrow.at[there], read.at[i]))
        reads[i].start()
    writes = []
    for i in range(PARTS):
        reads[i].wait()
        first = i * columns
        for j in range(first, first + columns):
            wide[:, j * 128:(j + 1) * 128] = narrow[j * HALF:(j + 1) * HALF, :].astype(F32)
        half, column = first // 16, first % 16
        if column < 8:
            there = up_out.at[:, pl.ds(half * QUARTER + column * 128, columns * 128)]
        else:
            there = down_out.at[pl.ds(half * QUARTER, QUARTER), pl.ds((column - 8) * 128, columns * 128)]
        writes.append(pltpu.make_async_copy(wide.at[:, pl.ds(first * 128, columns * 128)], there, write.at[i]))
        writes[i].start()
        if i == 0:
            through.wait()
            back = pltpu.make_async_copy(gin, gin_out, sem.at[1])
            back.start()
    back.wait()
    for copy in writes:
        copy.wait()


def shards(inputs, cotangent, w_up, w_down):
    vmem, anywhere = pl.BlockSpec(memory_space=pltpu.VMEM), pl.BlockSpec(memory_space=pl.ANY)
    gin_shape = jax.ShapeDtypeStruct((TOK, HALF), BF16)
    dma = pltpu.SemaphoreType.DMA
    grad_inputs, sums = pl.pallas_call(
        body,
        name="ffn_backward",
        out_shape=(gin_shape, jax.ShapeDtypeStruct((2 * ROWS, 128), BF16)),
        in_specs=[anywhere] * 4,
        out_specs=(vmem, anywhere),
        scratch_shapes=[
            pltpu.VMEM((TOK, HALF), BF16), pltpu.VMEM((TOK, HALF), BF16), pltpu.VMEM((2 * ROWS, 128), BF16),
            pltpu.VMEM((2 * GRP, HALF), BF16), pltpu.VMEM((2 * GRP, HALF), BF16),
            pltpu.VMEM((HALF, 2 * GRP), BF16), pltpu.VMEM((QUARTER, 2 * GRP), BF16),
            pltpu.VMEM((HALF, QUARTER), BF16), pltpu.VMEM((QUARTER, HALF), BF16),
            pltpu.VMEM((2 * NCH, GRP, CH), F32), pltpu.VMEM((2 * NCH, GRP, CH), F32),
            pltpu.VMEM((2 * NCH, GRP, CH), F32),
            pltpu.VMEM((2 * NCH, GRP, CH), BF16), pltpu.VMEM((2 * NCH, GRP, CH), BF16),
            pltpu.VMEM((2 * GRP, QUARTER), BF16), pltpu.VMEM((2 * GRP, QUARTER), BF16),
            pltpu.VMEM((ROWS, 128), BF16), pltpu.VMEM((LANDING, 128), BF16),
            pltpu.VMEM((2 * GRP, HALF), BF16), pltpu.VMEM((4, TOK, HALF), BF16),
            dma((4,)), dma((2, 3)), dma((2, 4)), dma((2, 2)), dma((4 * NCH,)), dma((4 * NCH,)),
            dma((2, 2)), dma((4,)), dma((len(TABLE),)), dma((len(TABLE),)), dma((2 * len(LANES),)),
        ],
        compiler_params=pltpu.CompilerParams(
            collective_id=0, has_side_effects=True, vmem_limit_bytes=60 * 2**20),
    )(inputs, cotangent, w_up, w_down)
    return pl.pallas_call(
        widen,
        name="widen",
        out_shape=(gin_shape, jax.ShapeDtypeStruct((HALF, HID), F32), jax.ShapeDtypeStruct((HID, HALF), F32)),
        in_specs=[anywhere] * 2,
        out_specs=(anywhere,) * 3,
        scratch_shapes=[
            pltpu.VMEM((TOK, HALF), BF16), pltpu.VMEM((2 * ROWS, 128), BF16),
            pltpu.VMEM((HALF, 2 * HID), F32),
            dma((2,)), dma((PARTS,)), dma((PARTS,)),
        ],
        compiler_params=pltpu.CompilerParams(vmem_limit_bytes=60 * 2**20),
    )(grad_inputs, sums)


def solution(mesh):
    return jax.shard_map(
        shards,
        mesh=mesh,
        in_specs=(P(("rep", "fs"), "tp"), P(("rep", "fs"), "tp"), P("fs", "tp"), P("tp", "fs")),
        out_specs=(P(("rep", "fs"), "tp"), P("fs", "tp"), P("tp", "fs")),
        check_vma=False,
    )
```

```python
import functools
import heapq

import jax
import jax.numpy as jnp
from jax import lax
from jax.experimental import pallas as pl
from jax.experimental.pallas import tpu as pltpu
from jax.sharding import PartitionSpec as P

MESH = pl.DeviceIdType.MESH
F32, BF16 = jnp.float32, jnp.bfloat16
NZ, NY, NX = 8, 4, 2
RINGS = {"y": NY, "z": NZ}
TOK, HALF, HID = 128, 1024, 2048
QUARTER = HID // 2
GRP = 2 * TOK
CH = 512
NCH = QUARTER // CH
ROWS = 2 * HALF * QUARTER // 128
TILE = 16
A, B = ("y", "z"), ("z", "y")
LANES = (
    (*A, 1, 2, True), (*B, -1, 2, True), (*A, -1, 3, True), (*B, 1, 2, True),
    (*A, 1, 3, True), (*B, -1, 2, False), (*A, -1, 3, False), (*A, 1, 3, False),
    (*B, 1, 2, False), (*A, -1, 2, False), (*B, 1, 2, False), (*A, 1, 2, False),
    (*B, 1, 2, False), (*B, -1, 2, False),
)
UPTO = tuple(sum(lane[3] for lane in LANES[:i + 1]) for i in range(len(LANES)))
STARTS = tuple(2.4 * tiles / 32 for tiles in UPTO)
PIECES = NY * NZ
RATE, LAG, WINDOW, WORK = 46000.0, 2.0, 1.6, 0.12
XFREE = 20.0
RANKS = {
    "rs1": (44, 18, 24, 107, 45, 37, 92, 14, 50, 77, 111, 62, 95, 110),
    "rs2": (27, 85, 11, 79, 84, 8, 80, 97, 83, 55, 87, 10, 93, 31),
    "x": (54, 75, 96, 39, 91, 104, 35, 63, 29, 34, 76, 82, 17, 43),
    "ag2": (49, 81, 9, 109, 12, 25, 66, 52, 51, 60, 101, 58, 53, 42),
    "ag1": (7, 67, 22, 90, 15, 86, 89, 40, 105, 108, 98, 57, 99, 74),
    "far2": (59, 78, 70, 65, 88, 69, 26, 6, 3, 19, 33, 0, 64, 1),
    "far1": (41, 56, 30, 48, 72, 100, 20, 13, 4, 68, 16, 71, 102, 2),
    "xl": (103, 36, 5, 47, 38, 46, 23, 32, 73, 61, 94, 21, 106, 28),
}
FIRST = ("rs1", "ag1", "far1", "xl")
SENDING = 24


def hops(n, arm):
    return n // 2 if arm == 0 else n // 2 - 1


def ring_of(lane, phase):
    return LANES[lane][0 if phase in FIRST else 1]


def length(lane, phase):
    piece = LANES[lane][3] * TILE
    return piece * RINGS[LANES[lane][1]] if phase in FIRST else piece


def last(lane, phase, arm, k):
    return phase == "x" or k == hops(RINGS[ring_of(lane, phase)], arm)


def way_of(lane, phase, arm):
    if phase in ("x", "xl"):
        return "x", 0
    way = LANES[lane][2] if arm == 0 else -LANES[lane][2]
    return ring_of(lane, phase), -way if phase[:2] == "rs" else way


def arrivals(lane, phase):
    n = RINGS[ring_of(lane, phase)]
    if phase == "x":
        return [(lane, phase, 0, 1)]
    if phase == "xl":
        return [(lane, phase, 0, 0)] + [(lane, phase, arm, k) for arm in (0, 1) for k in range(1, hops(n, arm) + 1)]
    if phase == "ag1" and LANES[lane][4]:
        return []
    return [(lane, phase, arm, hops(n, arm)) for arm in (0, 1)]


def planned():
    order, free, ready, flying, joined, now, count = [], {"x": XFREE}, {}, [], {}, 0.0, 0

    def want(lane, phase, arm, k):
        nonlocal count
        count += 1
        line = ready.setdefault(way_of(lane, phase, arm), [])
        heapq.heappush(line, (RANKS[phase][lane], -k, count, (lane, phase, arm, k)))

    def begin(lane, phase):
        joined[lane, phase] = 0
        for arm in (0,) if phase == "x" else (0, 1):
            want(lane, phase, arm, 1)

    def clear(link):
        return free.get("x" if link[0] == "x" else link, 0.0)

    def issue():
        nonlocal count
        for link, line in ready.items():
            while line and max(now, clear(link)) - now < WINDOW:
                what = heapq.heappop(line)[3]
                done = max(now, clear(link)) + length(what[0], what[1]) * 256 / RATE
                free["x" if link[0] == "x" else link] = done
                count += 1
                heapq.heappush(flying, (done + LAG, count, what))
                order.append(("send",) + what)

    todo = sorted((at, lane) for lane, at in enumerate(STARTS))
    while todo or flying:
        if todo and (not flying or todo[0][0] <= flying[0][0]):
            at, lane = todo.pop(0)
            now = max(now, at)
            order.append(("begin", lane))
            begin(lane, "rs1")
        else:
            at, _, (lane, phase, arm, k) = heapq.heappop(flying)
            now = max(now, at)
            late = LANES[lane][4]
            if phase == "xl":
                joined[lane, phase] += 1
                if joined[lane, phase] == RINGS[LANES[lane][0]]:
                    order.append(("end", lane, phase))
                    now += WORK
            elif late and phase == "ag1":
                now += WORK
                order.append(("pass", lane, phase, arm, k))
                if not last(lane, phase, arm, k):
                    want(lane, phase, arm, k + 1)
                else:
                    joined[lane, phase] += 1
                    if joined[lane, phase] == 2:
                        order.append(("end", lane, phase))
                want(lane, "xl", arm, k)
            elif not last(lane, phase, arm, k):
                now += WORK
                order.append(("pass", lane, phase, arm, k))
                want(lane, phase, arm, k + 1)
            else:
                joined[lane, phase] += 1
                if phase == "x" or joined[lane, phase] == 2:
                    now += WORK
                    order.append(("end", lane, phase))
                    for after in {"rs1": ("rs2",), "rs2": ("ag2",) if late else ("x", "ag2"), "x": ("far2",),
                                  "ag2": ("ag1",), "far2": ("far1",)}.get(phase, ()):
                        begin(lane, after)
                    if late and phase == "ag2":
                        joined[lane, "xl"] = 0
                        want(lane, "xl", 0, 0)
        issue()
        if not flying and not todo and any(ready.values()):
            now = min(clear(link) for link, line in ready.items() if line)
            issue()
    return order, now


ORDER, ESTIMATE = planned()


def transfers():
    sent, waited = {}, {}
    for at, step in enumerate(ORDER):
        if step[0] == "send":
            sent[step[1:]] = at
        elif step[0] == "pass":
            waited[step[1:]] = at
        elif step[0] == "end":
            waited.update((what, at) for what in arrivals(*step[1:]))
    table, rows, slots, back = {}, 0, [], {}
    for what in sent:
        back.setdefault(way_of(*what[:3]), []).append((sent[what], waited[what]))
    for what in sorted(sent, key=sent.get):
        ring, way = way_of(*what[:3])
        chosen = None
        for i, (link, free) in enumerate(slots):
            if link == (ring, way) and free < sent[what]:
                chosen = i
                break
        if chosen is None:
            chosen = len(slots)
            slots.append(None)
        heard = [end for begin, end in back[ring, -way] if begin > waited[what]]
        slots[chosen] = (ring, way), min(heard, default=len(ORDER))
        lands = what[1][:2] == "rs"
        table[what] = (chosen, rows if lands else None)
        rows += length(what[0], what[1]) if lands else 0
    return table, rows, len(slots)


TABLE, LANDING, RECEIVING = transfers()


def dot(a, b, dims):
    return lax.dot_general(a, b, (dims, ((), ())), preferred_element_type=F32)


def body(in_ref, cot_ref, up_ref, down_ref, gin_ref, sums_ref,
         in_v, cot_v, out_ref, x, c, xt, sqt, up, down, p_own, p_far, a_own, a_out, a_far, pre, sq, g, land, r, r_in,
         local_sem, xs, xr, fsem, ds, dr, gs, gr, ss, rs, os):
    rep, f, t = lax.axis_index("rep"), lax.axis_index("fs"), lax.axis_index("tp")
    xh = lax.rem(rep, NX)
    yz = rep // NX
    xpos = xh * 2 + t
    pos = {"y": lax.rem(yz, NY), "z": yz // NY}

    def at(ring, step):
        n = RINGS[ring]
        there = dict(pos)
        there[ring] = lax.rem(pos[ring] + step + n, n)
        return ((there["z"] * NY + there["y"]) * NX + xh, f, t)

    def along(step, who):
        there = lax.rem(xpos + step + 4, 4)
        return (yz * NX + there // 2, who, lax.rem(there, 2))

    core = (rep, 1 - f, t)
    xpeer = (yz * NX + 1 - xh, f, t)
    home = f == t
    away = jnp.logical_not(home)

    share = pl.ds(pl.multiple_of(xh * QUARTER, QUARTER), QUARTER)
    w_copies = [pltpu.make_async_copy(up_ref.at[:, share], up, local_sem.at[0]),
                pltpu.make_async_copy(down_ref.at[share, :], down, local_sem.at[1])]
    t_copies = [pltpu.make_async_copy(in_ref, in_v, local_sem.at[2]),
                pltpu.make_async_copy(cot_ref, cot_v, local_sem.at[3])]
    for copy in t_copies + w_copies:
        copy.start()

    barrier = pltpu.get_barrier_semaphore()
    partners = [core] + [along(step, who) for step in (1, -1, 2) for who in (0, 1)] + [
        at("y", 1), at("y", -1), at("z", 1), at("z", -1)]
    for who in partners:
        pl.semaphore_signal(barrier, inc=1, device_id=who, device_id_type=MESH)
    pl.semaphore_wait(barrier, len(partners))

    def remote(src, dst, send, recv, who):
        return pltpu.make_async_remote_copy(
            src_ref=src, dst_ref=dst, send_sem=send, recv_sem=recv, device_id=who, device_id_type=MESH)

    def block(group, who):
        return pl.ds(pl.multiple_of((group * 2 + who) * TOK, TOK), TOK)

    pairs = ((in_v, x), (cot_v, c))

    def across(i, way):
        src, dst = pairs[i]
        group = t if way == 1 else 1 - t
        return remote(src, dst.at[block(group, f)], xs.at[i, 0 if way == 1 else 1],
                      xr.at[i, group * 2 + f], along(way, t))

    def beside(i):
        src, dst = pairs[i]
        return remote(src, dst.at[block(0, f)], xs.at[i, 2], xr.at[i, f], core)

    def onward(i, way):
        _, dst = pairs[i]
        group, who = (1 - t, 0) if way == 1 else (t, 1)
        return remote(dst.at[block(group, who)], dst.at[block(1, who)], fsem.at[i, who],
                      xr.at[i, 2 + who], along(way, f))

    def landed(i, group, who):
        _, dst = pairs[i]
        there = dst.at[block(group, who)]
        remote(there, there, xs.at[i, 0], xr.at[i, group * 2 + who], core).wait_recv()

    for i in (0, 1):
        t_copies[i].wait()
        across(i, 1).start()
        across(i, -1).start()
        src, dst = pairs[i]

        @pl.when(home)
        def _():
            dst[block(0, f), :] = src[...]

        @pl.when(away)
        def _():
            beside(i).start()

    def pass_on(i):
        @pl.when(away)
        def _():
            landed(i, 1 - t, 0)
            onward(i, 1).start()
            landed(i, t, 1)
            onward(i, -1).start()

    def arrive(i, group):
        if group == 0:
            @pl.when(home)
            def _():
                landed(i, 0, 1 - f)
        else:
            @pl.when(home)
            def _():
                landed(i, 1, 0)
                landed(i, 1, 1)

        @pl.when(away)
        def _():
            landed(i, group, jnp.where(group == t, 0, 1))

    def swap_p(i):
        return remote(p_own.at[i], p_far.at[i], ds.at[i], dr.at[i], core)

    def swap_a(i):
        return remote(a_out.at[i], a_far.at[i], ds.at[2 * NCH + i], dr.at[2 * NCH + i], core)

    def first_product(group):
        arrive(0, group)
        here = pl.ds(group * GRP, GRP)
        for j in range(NCH):
            i = group * NCH + j
            p_own[i] = dot(x[here, :], up[:, j * CH:(j + 1) * CH], ((1,), (0,)))
            swap_p(i).start()
        xt[:, here] = x[here, :].T

    def second_product(group):
        arrive(1, group)
        here = pl.ds(group * GRP, GRP)
        for j in range(NCH):
            i = group * NCH + j
            part = dot(c[here, :], down[j * CH:(j + 1) * CH, :], ((1,), (1,)))
            a_own[i] = part
            a_out[i] = part.astype(BF16)
            swap_a(i).start()

    pass_on(0)
    for w in w_copies:
        w.wait()
    first_product(0)
    pass_on(1)
    second_product(0)
    first_product(1)
    second_product(1)

    def activations(j):
        cols = slice(j * CH, (j + 1) * CH)
        for group in (0, 1):
            i = group * NCH + j
            swap_p(i).wait_recv()
            swap_a(i).wait_recv()
            here = slice(group * GRP, (group + 1) * GRP)
            relu = jnp.maximum(p_own[i] + p_far[i], 0.0)
            sq[here, cols] = (relu * relu).astype(BF16)
            grad = a_own[i] + a_far[i].astype(F32)
            pre[here, cols] = (2.0 * relu * grad).astype(BF16)

    def local_up(j):
        activations(j)
        part = dot(xt[...], pre[:, j * CH:(j + 1) * CH], ((1,), (0,)))
        for k in range(CH // 128):
            g[(j * 4 + k) * HALF:(j * 4 + k + 1) * HALF, :] = part[:, k * 128:(k + 1) * 128].astype(BF16)

    def local_down(j):
        if j == 0:
            sqt[...] = sq[...].T
        part = dot(sqt[...], c[:, j * CH:(j + 1) * CH], ((1,), (0,)))
        for k in range(CH // 128):
            g[(8 + j * 4 + k) * HALF:(9 + j * 4 + k) * HALF, :] = part[:, k * 128:(k + 1) * 128].astype(BF16)

    def inputs_part(j):
        rows = slice(j * 256, (j + 1) * 256)
        r[:, rows] = dot(pre[...], up[rows, :], ((1,), (1,))).astype(BF16)

    def give(group, who):
        there = jnp.where(group == 0, xh, 1 - xh)
        return remote(r.at[block(group, who)], r_in.at[xpos], gs.at[group, who], gr.at[xpos],
                      (yz * NX + there, who, f))

    def give_all():
        @pl.when(home)
        def _():
            give(0, 1 - f).start()
            r_in[xpos] = r[block(0, f), :]

        @pl.when(away)
        def _():
            give(0, f).start()
            give(0, 1 - f).start()

        give(1, 0).start()
        give(1, 1).start()

    def inputs_sum():
        def came(k):
            there = r_in.at[k]
            remote(there, there, gs.at[0, 0], gr.at[k], core).wait_recv()

        @pl.when(away)
        def _():
            came(xpos)

        for step in (1, 2, 3):
            came(lax.rem(xpos + step, 4))
        total = r_in[0].astype(F32)
        for k in range(1, 4):
            total += r_in[k].astype(F32)
        gin_ref[...] = total.astype(BF16)

    bases, base = [], 0
    for lane in range(len(LANES)):
        bases.append(base)
        base += LANES[lane][3] * TILE * PIECES
    started, outgoing = {}, []

    def chunk(lane, phase, step):
        ring = ring_of(lane, phase)
        rows = length(lane, phase)
        start = bases[lane]
        if phase not in FIRST:
            start += pos[LANES[lane][0]] * length(lane, "rs1")
        if phase[:2] == "ag" or phase in ("x", "xl"):
            start += xh * ROWS
        elif phase[:3] == "far":
            start += (1 - xh) * ROWS
        n = RINGS[ring]
        there = lax.rem(pos[ring] + LANES[lane][2] * step + n, n)
        return pl.multiple_of(start + there * rows, TILE), rows

    def send(lane, phase, arm, k):
        index, slot = TABLE[lane, phase, arm, k]
        ring = ring_of(lane, phase)
        way = LANES[lane][2] if arm == 0 else -LANES[lane][2]
        if phase == "x":
            begin, rows = chunk(lane, phase, 0)
            src = dst = out_ref.at[pl.ds(begin, rows)]
            who = xpeer
        elif phase == "xl":
            begin, rows = chunk(lane, phase, -k if arm == 0 else k)
            src = dst = out_ref.at[pl.ds(begin, rows)]
            who = xpeer
        elif slot is not None:
            left = hops(RINGS[ring], arm) - k + 1
            begin, rows = chunk(lane, phase, -left if arm == 0 else left)
            src, dst, who = g.at[pl.ds(begin, rows)], land.at[pl.ds(slot, rows)], at(ring, -way)
        else:
            begin, rows = chunk(lane, phase, 1 - k if arm == 0 else k - 1)
            src = dst = out_ref.at[pl.ds(begin, rows)]
            who = at(ring, way)
        if len(outgoing) >= SENDING:
            outgoing[-SENDING].wait_send()
        copy = remote(src, dst, ss.at[len(outgoing) % SENDING], rs.at[index], who)
        copy.start()
        outgoing.append(copy)
        started[lane, phase, arm, k] = copy

    def add(target, shift, begin, slots, rows):
        unit = max(u for u in range(TILE, 193, TILE) if rows % u == 0)

        @pl.loop(0, rows // unit)
        def _(i):
            here = pl.multiple_of(begin + i * unit, TILE)
            total = g[pl.ds(here, unit), :].astype(F32)
            for slot in slots:
                total += land[pl.ds(pl.multiple_of(slot + i * unit, TILE), unit), :].astype(F32)
            target[pl.ds(pl.multiple_of(here + shift, TILE), unit), :] = total.astype(BF16)

    aside = [functools.partial(inputs_part, j) for j in range(4)] + [give_all]
    leaving = []
    begun = chunks = 0
    for count, step in enumerate(ORDER):
        kind, lane = step[:2]
        if kind == "begin":
            begun += 1
            while chunks * 8 < UPTO[lane]:
                (local_up, local_down)[chunks // 2](chunks % 2)
                chunks += 1
        elif kind == "send":
            send(*step[1:])
        elif kind == "pass":
            phase, arm, k = step[2:]
            started[lane, phase, arm, k].wait_recv()
            if phase[:2] == "rs":
                left = hops(RINGS[ring_of(lane, phase)], arm) - k
                begin, rows = chunk(lane, phase, -left if arm == 0 else left)
                add(g, 0, begin, (TABLE[lane, phase, arm, k][1],), rows)
            if begun == len(LANES) and aside:
                aside.pop(0)()
        else:
            phase = step[2]
            ends = arrivals(lane, phase)
            for which in ends:
                started[which].wait_recv()
            if phase[:2] == "rs":
                begin, rows = chunk(lane, phase, 0)
                into, shift = (g, 0) if phase == "rs1" else (out_ref, xh * ROWS)
                add(into, shift, begin, [TABLE[which][1] for which in ends], rows)
            elif phase in ("ag1", "far1", "xl"):
                half = xh if phase == "ag1" else 1 - xh
                there = pl.ds(pl.multiple_of(half * ROWS + bases[lane], TILE), LANES[lane][3] * TILE * PIECES)
                if len(leaving) >= 4:
                    leaving[-4].wait()
                leaving.append(pltpu.make_async_copy(
                    out_ref.at[there], sums_ref.at[there], os.at[len(leaving) % 4]))
                leaving[-1].start()
        if count == len(ORDER) * 3 // 5:
            inputs_sum()

    for i in (0, 1):
        across(i, 1).wait_send()
        across(i, -1).wait_send()

        @pl.when(away)
        def _():
            beside(i).wait_send()
            onward(i, 1).wait_send()
            onward(i, -1).wait_send()
    for i in range(2 * NCH):
        swap_p(i).wait_send()
        swap_a(i).wait_send()

    give(0, 1 - f).wait_send()
    give(1, 0).wait_send()
    give(1, 1).wait_send()

    @pl.when(away)
    def _():
        give(0, f).wait_send()
    for copy in outgoing[-SENDING:]:
        copy.wait_send()
    for copy in leaving[-4:]:
        copy.wait()


PARTS = 8


def widen(gin_ref, sums_ref, gin_out, up_out, down_out, gin, narrow, wide, sem, read, write):
    through = pltpu.make_async_copy(gin_ref, gin, sem.at[0])
    through.start()
    rows, columns = 2 * ROWS // PARTS, 2 * ROWS // PARTS // HALF
    reads = []
    for i in range(PARTS):
        there = pl.ds(i * rows, rows)
        reads.append(pltpu.make_async_copy(sums_ref.at[there], narrow.at[there], read.at[i]))
        reads[i].start()
    writes = []
    for i in range(PARTS):
        reads[i].wait()
        first = i * columns
        for j in range(first, first + columns):
            wide[:, j * 128:(j + 1) * 128] = narrow[j * HALF:(j + 1) * HALF, :].astype(F32)
        half, column = first // 16, first % 16
        if column < 8:
            there = up_out.at[:, pl.ds(half * QUARTER + column * 128, columns * 128)]
        else:
            there = down_out.at[pl.ds(half * QUARTER, QUARTER), pl.ds((column - 8) * 128, columns * 128)]
        writes.append(pltpu.make_async_copy(wide.at[:, pl.ds(first * 128, columns * 128)], there, write.at[i]))
        writes[i].start()
        if i == 0:
            through.wait()
            back = pltpu.make_async_copy(gin, gin_out, sem.at[1])
            back.start()
    back.wait()
    for copy in writes:
        copy.wait()


def shards(inputs, cotangent, w_up, w_down):
    vmem, anywhere = pl.BlockSpec(memory_space=pltpu.VMEM), pl.BlockSpec(memory_space=pl.ANY)
    gin_shape = jax.ShapeDtypeStruct((TOK, HALF), BF16)
    dma = pltpu.SemaphoreType.DMA
    grad_inputs, sums = pl.pallas_call(
        body,
        name="ffn_backward",
        out_shape=(gin_shape, jax.ShapeDtypeStruct((2 * ROWS, 128), BF16)),
        in_specs=[anywhere] * 4,
        out_specs=(vmem, anywhere),
        scratch_shapes=[
            pltpu.VMEM((TOK, HALF), BF16), pltpu.VMEM((TOK, HALF), BF16), pltpu.VMEM((2 * ROWS, 128), BF16),
            pltpu.VMEM((2 * GRP, HALF), BF16), pltpu.VMEM((2 * GRP, HALF), BF16),
            pltpu.VMEM((HALF, 2 * GRP), BF16), pltpu.VMEM((QUARTER, 2 * GRP), BF16),
            pltpu.VMEM((HALF, QUARTER), BF16), pltpu.VMEM((QUARTER, HALF), BF16),
            pltpu.VMEM((2 * NCH, GRP, CH), F32), pltpu.VMEM((2 * NCH, GRP, CH), F32),
            pltpu.VMEM((2 * NCH, GRP, CH), F32),
            pltpu.VMEM((2 * NCH, GRP, CH), BF16), pltpu.VMEM((2 * NCH, GRP, CH), BF16),
            pltpu.VMEM((2 * GRP, QUARTER), BF16), pltpu.VMEM((2 * GRP, QUARTER), BF16),
            pltpu.VMEM((ROWS, 128), BF16), pltpu.VMEM((LANDING, 128), BF16),
            pltpu.VMEM((2 * GRP, HALF), BF16), pltpu.VMEM((4, TOK, HALF), BF16),
            dma((4,)), dma((2, 3)), dma((2, 4)), dma((2, 2)), dma((4 * NCH,)), dma((4 * NCH,)),
            dma((2, 2)), dma((4,)), dma((SENDING,)), dma((RECEIVING,)), dma((4,)),
        ],
        compiler_params=pltpu.CompilerParams(
            collective_id=0, has_side_effects=True, vmem_limit_bytes=60 * 2**20),
    )(inputs, cotangent, w_up, w_down)
    return pl.pallas_call(
        widen,
        name="widen",
        out_shape=(gin_shape, jax.ShapeDtypeStruct((HALF, HID), F32), jax.ShapeDtypeStruct((HID, HALF), F32)),
        in_specs=[anywhere] * 2,
        out_specs=(anywhere,) * 3,
        scratch_shapes=[
            pltpu.VMEM((TOK, HALF), BF16), pltpu.VMEM((2 * ROWS, 128), BF16),
            pltpu.VMEM((HALF, 2 * HID), F32),
            dma((2,)), dma((PARTS,)), dma((PARTS,)),
        ],
        compiler_params=pltpu.CompilerParams(vmem_limit_bytes=60 * 2**20),
    )(grad_inputs, sums)


def solution(mesh):
    return jax.shard_map(
        shards,
        mesh=mesh,
        in_specs=(P(("rep", "fs"), "tp"), P(("rep", "fs"), "tp"), P("fs", "tp"), P("tp", "fs")),
        out_specs=(P(("rep", "fs"), "tp"), P("fs", "tp"), P("tp", "fs")),
        check_vma=False,
    )
```

```python
import functools
import heapq

import jax
import jax.numpy as jnp
from jax import lax
from jax.experimental import pallas as pl
from jax.experimental.pallas import tpu as pltpu
from jax.sharding import PartitionSpec as P

MESH = pl.DeviceIdType.MESH
F32, BF16 = jnp.float32, jnp.bfloat16
NZ, NY, NX = 8, 4, 2
RINGS = {"y": NY, "z": NZ}
TOK, HALF, HID = 128, 1024, 2048
QUARTER = HID // 2
GRP = 2 * TOK
CH = 512
NCH = QUARTER // CH
ROWS = 2 * HALF * QUARTER // 128
TILE = 16
A, B = ("y", "z"), ("z", "y")
LANES = (
    (*B, -1, 2, True), (*B, 1, 2, True), (*A, -1, 2, False), (*B, -1, 2, False),
    (*A, 1, 2, True), (*A, 1, 2, False), (*B, 1, 2, False), (*B, 1, 2, False),
    (*B, -1, 2, False), (*A, 1, 2, False), (*B, 1, 2, False), (*A, 1, 2, True),
    (*A, -1, 2, False), (*A, -1, 2, False), (*A, 1, 2, True), (*A, -1, 2, True),
)
UPTO = tuple(sum(lane[3] for lane in LANES[:i + 1]) for i in range(len(LANES)))
STARTS = tuple(2.4 * tiles / 32 for tiles in UPTO)
PIECES = NY * NZ
RATE, LAG, WINDOW, WORK = 46000.0, 2.0, 1.2, 0.12
XFREE = 20.0
RANKS = {
    "rs1": (15, 121, 3, 111, 7, 93, 115, 43, 98, 65, 127, 92, 23, 49, 55, 12),
    "rs2": (71, 8, 37, 95, 125, 78, 85, 126, 0, 76, 17, 107, 84, 68, 32, 29),
    "x": (91, 73, 57, 74, 39, 24, 105, 103, 34, 81, 62, 59, 83, 75, 53, 42),
    "ag2": (99, 72, 101, 94, 88, 64, 100, 56, 30, 20, 120, 67, 16, 11, 33, 45),
    "ag1": (19, 96, 90, 119, 1, 52, 28, 108, 87, 38, 110, 35, 89, 9, 50, 10),
    "far2": (4, 69, 82, 77, 80, 46, 66, 70, 116, 60, 31, 5, 2, 14, 51, 102),
    "far1": (40, 124, 97, 113, 117, 41, 109, 27, 112, 122, 79, 47, 118, 21, 44, 54),
    "xl": (114, 106, 86, 25, 18, 61, 26, 104, 63, 6, 22, 123, 36, 13, 58, 48),
}
FIRST = ("rs1", "ag1", "far1", "xl")
SENDING = 24


def hops(n, arm):
    return n // 2 if arm == 0 else n // 2 - 1


def ring_of(lane, phase):
    return LANES[lane][0 if phase in FIRST else 1]


def length(lane, phase):
    piece = LANES[lane][3] * TILE
    return piece * RINGS[LANES[lane][1]] if phase in FIRST else piece


def lane_rows(lane):
    return LANES[lane][3] * TILE * PIECES


def last(lane, phase, arm, k):
    return phase == "x" or k == hops(RINGS[ring_of(lane, phase)], arm)


def way_of(lane, phase, arm):
    if phase in ("x", "xl"):
        return "x", 0
    way = LANES[lane][2] if arm == 0 else -LANES[lane][2]
    return ring_of(lane, phase), -way if phase[:2] == "rs" else way


def arrivals(lane, phase):
    n = RINGS[ring_of(lane, phase)]
    if phase == "x":
        return [(lane, phase, 0, 1)]
    if phase == "xl":
        return [(lane, phase, 0, 0)] + [(lane, phase, arm, k) for arm in (0, 1) for k in range(1, hops(n, arm) + 1)]
    if phase == "ag1" and LANES[lane][4]:
        return []
    return [(lane, phase, arm, hops(n, arm)) for arm in (0, 1)]


def planned():
    order, free, ready, flying, joined, now, count = [], {"x": XFREE}, {}, [], {}, 0.0, 0

    def want(lane, phase, arm, k):
        nonlocal count
        count += 1
        line = ready.setdefault(way_of(lane, phase, arm), [])
        heapq.heappush(line, (RANKS[phase][lane], -k, count, (lane, phase, arm, k)))

    def begin(lane, phase):
        joined[lane, phase] = 0
        for arm in (0,) if phase == "x" else (0, 1):
            want(lane, phase, arm, 1)

    def clear(link):
        return free.get("x" if link[0] == "x" else link, 0.0)

    def issue():
        nonlocal count
        for link, line in ready.items():
            while line and max(now, clear(link)) - now < WINDOW:
                what = heapq.heappop(line)[3]
                done = max(now, clear(link)) + length(what[0], what[1]) * 256 / RATE
                free["x" if link[0] == "x" else link] = done
                count += 1
                heapq.heappush(flying, (done + LAG, count, what))
                order.append(("send",) + what)

    todo = sorted((at, lane) for lane, at in enumerate(STARTS))
    while todo or flying:
        if todo and (not flying or todo[0][0] <= flying[0][0]):
            at, lane = todo.pop(0)
            now = max(now, at)
            order.append(("begin", lane))
            begin(lane, "rs1")
        else:
            at, _, (lane, phase, arm, k) = heapq.heappop(flying)
            now = max(now, at)
            late = LANES[lane][4]
            if phase == "xl":
                joined[lane, phase] += 1
                if joined[lane, phase] == RINGS[LANES[lane][0]]:
                    order.append(("end", lane, phase))
                    now += WORK
            elif late and phase == "ag1":
                now += WORK
                order.append(("pass", lane, phase, arm, k))
                if not last(lane, phase, arm, k):
                    want(lane, phase, arm, k + 1)
                else:
                    joined[lane, phase] += 1
                    if joined[lane, phase] == 2:
                        order.append(("end", lane, phase))
                want(lane, "xl", arm, k)
            elif not last(lane, phase, arm, k):
                now += WORK
                order.append(("pass", lane, phase, arm, k))
                want(lane, phase, arm, k + 1)
            else:
                joined[lane, phase] += 1
                if phase == "x" or joined[lane, phase] == 2:
                    now += WORK
                    order.append(("end", lane, phase))
                    for after in {"rs1": ("rs2",), "rs2": ("ag2",) if late else ("x", "ag2"), "x": ("far2",),
                                  "ag2": ("ag1",), "far2": ("far1",)}.get(phase, ()):
                        begin(lane, after)
                    if late and phase == "ag2":
                        joined[lane, "xl"] = 0
                        want(lane, "xl", 0, 0)
        issue()
        if not flying and not todo and any(ready.values()):
            now = min(clear(link) for link, line in ready.items() if line)
            issue()
    return order, now


ORDER, ESTIMATE = planned()


def transfers():
    sent, waited = {}, {}
    for at, step in enumerate(ORDER):
        if step[0] == "send":
            sent[step[1:]] = at
        elif step[0] == "pass":
            waited[step[1:]] = at
        elif step[0] == "end":
            waited.update((what, at) for what in arrivals(*step[1:]))
    table, rows, slots, back = {}, 0, [], {}
    for what in sent:
        back.setdefault(way_of(*what[:3]), []).append((sent[what], waited[what]))
    for what in sorted(sent, key=sent.get):
        ring, way = way_of(*what[:3])
        chosen = None
        for i, (link, free) in enumerate(slots):
            if link == (ring, way) and free < sent[what]:
                chosen = i
                break
        if chosen is None:
            chosen = len(slots)
            slots.append(None)
        heard = [end for begin, end in back[ring, -way] if begin > waited[what]]
        slots[chosen] = (ring, way), min(heard, default=len(ORDER))
        lands = what[1][:2] == "rs"
        table[what] = (chosen, rows if lands else None)
        rows += length(what[0], what[1]) if lands else 0
    return table, rows, len(slots)


TABLE, LANDING, RECEIVING = transfers()


def dot(a, b, dims):
    return lax.dot_general(a, b, (dims, ((), ())), preferred_element_type=F32)


def body(in_ref, cot_ref, up_ref, down_ref, gin_ref, *refs):
    outs = refs[:len(LANES)]
    (in_v, cot_v, x, c, xt, sqt, up, down, p_own, p_far, a_own, a_out, a_far, pre, sq, g, land, r, r_in,
     local_sem, xs, xr, fsem, ds, dr, gs, gr, ss, rs) = refs[len(LANES):]
    rep, f, t = lax.axis_index("rep"), lax.axis_index("fs"), lax.axis_index("tp")
    xh = lax.rem(rep, NX)
    yz = rep // NX
    xpos = xh * 2 + t
    pos = {"y": lax.rem(yz, NY), "z": yz // NY}

    def at(ring, step):
        n = RINGS[ring]
        there = dict(pos)
        there[ring] = lax.rem(pos[ring] + step + n, n)
        return ((there["z"] * NY + there["y"]) * NX + xh, f, t)

    def along(step, who):
        there = lax.rem(xpos + step + 4, 4)
        return (yz * NX + there // 2, who, lax.rem(there, 2))

    core = (rep, 1 - f, t)
    xpeer = (yz * NX + 1 - xh, f, t)
    home = f == t
    away = jnp.logical_not(home)

    share = pl.ds(pl.multiple_of(xh * QUARTER, QUARTER), QUARTER)
    w_copies = [pltpu.make_async_copy(up_ref.at[:, share], up, local_sem.at[0]),
                pltpu.make_async_copy(down_ref.at[share, :], down, local_sem.at[1])]
    t_copies = [pltpu.make_async_copy(in_ref, in_v, local_sem.at[2]),
                pltpu.make_async_copy(cot_ref, cot_v, local_sem.at[3])]
    for copy in t_copies + w_copies:
        copy.start()

    barrier = pltpu.get_barrier_semaphore()
    partners = [core] + [along(step, who) for step in (1, -1, 2) for who in (0, 1)] + [
        at("y", 1), at("y", -1), at("z", 1), at("z", -1)]
    for who in partners:
        pl.semaphore_signal(barrier, inc=1, device_id=who, device_id_type=MESH)
    pl.semaphore_wait(barrier, len(partners))

    def remote(src, dst, send, recv, who):
        return pltpu.make_async_remote_copy(
            src_ref=src, dst_ref=dst, send_sem=send, recv_sem=recv, device_id=who, device_id_type=MESH)

    def block(group, who):
        return pl.ds(pl.multiple_of((group * 2 + who) * TOK, TOK), TOK)

    pairs = ((in_v, x), (cot_v, c))

    def across(i, way):
        src, dst = pairs[i]
        group = t if way == 1 else 1 - t
        return remote(src, dst.at[block(group, f)], xs.at[i, 0 if way == 1 else 1],
                      xr.at[i, group * 2 + f], along(way, t))

    def beside(i):
        src, dst = pairs[i]
        return remote(src, dst.at[block(0, f)], xs.at[i, 2], xr.at[i, f], core)

    def onward(i, way):
        _, dst = pairs[i]
        group, who = (1 - t, 0) if way == 1 else (t, 1)
        return remote(dst.at[block(group, who)], dst.at[block(1, who)], fsem.at[i, who],
                      xr.at[i, 2 + who], along(way, f))

    def landed(i, group, who):
        _, dst = pairs[i]
        there = dst.at[block(group, who)]
        remote(there, there, xs.at[i, 0], xr.at[i, group * 2 + who], core).wait_recv()

    for i in (0, 1):
        t_copies[i].wait()
        across(i, 1).start()
        across(i, -1).start()
        src, dst = pairs[i]

        @pl.when(home)
        def _():
            dst[block(0, f), :] = src[...]

        @pl.when(away)
        def _():
            beside(i).start()

    def pass_on(i):
        @pl.when(away)
        def _():
            landed(i, 1 - t, 0)
            onward(i, 1).start()
            landed(i, t, 1)
            onward(i, -1).start()

    def arrive(i, group):
        if group == 0:
            @pl.when(home)
            def _():
                landed(i, 0, 1 - f)
        else:
            @pl.when(home)
            def _():
                landed(i, 1, 0)
                landed(i, 1, 1)

        @pl.when(away)
        def _():
            landed(i, group, jnp.where(group == t, 0, 1))

    def swap_p(i):
        return remote(p_own.at[i], p_far.at[i], ds.at[i], dr.at[i], core)

    def swap_a(i):
        return remote(a_out.at[i], a_far.at[i], ds.at[2 * NCH + i], dr.at[2 * NCH + i], core)

    def first_product(group):
        arrive(0, group)
        here = pl.ds(group * GRP, GRP)
        for j in range(NCH):
            i = group * NCH + j
            p_own[i] = dot(x[here, :], up[:, j * CH:(j + 1) * CH], ((1,), (0,)))
            swap_p(i).start()
        xt[:, here] = x[here, :].T

    def second_product(group):
        arrive(1, group)
        here = pl.ds(group * GRP, GRP)
        for j in range(NCH):
            i = group * NCH + j
            part = dot(c[here, :], down[j * CH:(j + 1) * CH, :], ((1,), (1,)))
            a_own[i] = part
            a_out[i] = part.astype(BF16)
            swap_a(i).start()

    pass_on(0)
    for w in w_copies:
        w.wait()
    first_product(0)
    pass_on(1)
    second_product(0)
    first_product(1)
    second_product(1)

    def activations(j):
        cols = slice(j * CH, (j + 1) * CH)
        for group in (0, 1):
            i = group * NCH + j
            swap_p(i).wait_recv()
            swap_a(i).wait_recv()
            here = slice(group * GRP, (group + 1) * GRP)
            relu = jnp.maximum(p_own[i] + p_far[i], 0.0)
            sq[here, cols] = (relu * relu).astype(BF16)
            grad = a_own[i] + a_far[i].astype(F32)
            pre[here, cols] = (2.0 * relu * grad).astype(BF16)

    def local_up(j):
        activations(j)
        part = dot(xt[...], pre[:, j * CH:(j + 1) * CH], ((1,), (0,)))
        for k in range(CH // 128):
            g[(j * 4 + k) * HALF:(j * 4 + k + 1) * HALF, :] = part[:, k * 128:(k + 1) * 128].astype(BF16)

    def local_down(j):
        if j == 0:
            sqt[...] = sq[...].T
        part = dot(sqt[...], c[:, j * CH:(j + 1) * CH], ((1,), (0,)))
        for k in range(CH // 128):
            g[(8 + j * 4 + k) * HALF:(9 + j * 4 + k) * HALF, :] = part[:, k * 128:(k + 1) * 128].astype(BF16)

    def inputs_part(j):
        rows = slice(j * 256, (j + 1) * 256)
        r[:, rows] = dot(pre[...], up[rows, :], ((1,), (1,))).astype(BF16)

    def give(group, who):
        there = jnp.where(group == 0, xh, 1 - xh)
        return remote(r.at[block(group, who)], r_in.at[xpos], gs.at[group, who], gr.at[xpos],
                      (yz * NX + there, who, f))

    def give_all():
        @pl.when(home)
        def _():
            give(0, 1 - f).start()
            r_in[xpos] = r[block(0, f), :]

        @pl.when(away)
        def _():
            give(0, f).start()
            give(0, 1 - f).start()

        give(1, 0).start()
        give(1, 1).start()

    def inputs_sum():
        def came(k):
            there = r_in.at[k]
            remote(there, there, gs.at[0, 0], gr.at[k], core).wait_recv()

        @pl.when(away)
        def _():
            came(xpos)

        for step in (1, 2, 3):
            came(lax.rem(xpos + step, 4))
        total = r_in[0].astype(F32)
        for k in range(1, 4):
            total += r_in[k].astype(F32)
        gin_ref[...] = total.astype(BF16)

    bases, base = [], 0
    for lane in range(len(LANES)):
        bases.append(base)
        base += LANES[lane][3] * TILE * PIECES
    started, outgoing = {}, []

    def chunk(lane, phase, step):
        ring = ring_of(lane, phase)
        rows = length(lane, phase)
        if phase[:2] == "rs":
            start = bases[lane]
        elif phase[:3] == "far":
            start = (1 - xh) * lane_rows(lane)
        else:
            start = xh * lane_rows(lane)
        if phase not in FIRST:
            start += pos[LANES[lane][0]] * length(lane, "rs1")
        n = RINGS[ring]
        there = lax.rem(pos[ring] + LANES[lane][2] * step + n, n)
        return pl.multiple_of(start + there * rows, TILE), rows

    def send(lane, phase, arm, k):
        index, slot = TABLE[lane, phase, arm, k]
        ring = ring_of(lane, phase)
        way = LANES[lane][2] if arm == 0 else -LANES[lane][2]
        if phase == "x":
            begin, rows = chunk(lane, phase, 0)
            src = dst = outs[lane].at[pl.ds(begin, rows)]
            who = xpeer
        elif phase == "xl":
            begin, rows = chunk(lane, phase, -k if arm == 0 else k)
            src = dst = outs[lane].at[pl.ds(begin, rows)]
            who = xpeer
        elif slot is not None:
            left = hops(RINGS[ring], arm) - k + 1
            begin, rows = chunk(lane, phase, -left if arm == 0 else left)
            src, dst, who = g.at[pl.ds(begin, rows)], land.at[pl.ds(slot, rows)], at(ring, -way)
        else:
            begin, rows = chunk(lane, phase, 1 - k if arm == 0 else k - 1)
            src = dst = outs[lane].at[pl.ds(begin, rows)]
            who = at(ring, way)
        if len(outgoing) >= SENDING:
            outgoing[-SENDING].wait_send()
        copy = remote(src, dst, ss.at[len(outgoing) % SENDING], rs.at[index], who)
        copy.start()
        outgoing.append(copy)
        started[lane, phase, arm, k] = copy

    def add(target, shift, begin, slots, rows):
        unit = max(u for u in range(TILE, 193, TILE) if rows % u == 0)

        @pl.loop(0, rows // unit)
        def _(i):
            here = pl.multiple_of(begin + i * unit, TILE)
            total = g[pl.ds(here, unit), :].astype(F32)
            for slot in slots:
                total += land[pl.ds(pl.multiple_of(slot + i * unit, TILE), unit), :].astype(F32)
            target[pl.ds(pl.multiple_of(here + shift, TILE), unit), :] = total.astype(BF16)

    aside = [functools.partial(inputs_part, j) for j in range(4)] + [give_all]
    begun = chunks = 0
    for count, step in enumerate(ORDER):
        kind, lane = step[:2]
        if kind == "begin":
            begun += 1
            while chunks * 8 < UPTO[lane]:
                (local_up, local_down)[chunks // 2](chunks % 2)
                chunks += 1
        elif kind == "send":
            send(*step[1:])
        elif kind == "pass":
            phase, arm, k = step[2:]
            started[lane, phase, arm, k].wait_recv()
            if phase[:2] == "rs":
                left = hops(RINGS[ring_of(lane, phase)], arm) - k
                begin, rows = chunk(lane, phase, -left if arm == 0 else left)
                add(g, 0, begin, (TABLE[lane, phase, arm, k][1],), rows)
            if begun == len(LANES) and aside:
                aside.pop(0)()
        else:
            phase = step[2]
            ends = arrivals(lane, phase)
            for which in ends:
                started[which].wait_recv()
            if phase[:2] == "rs":
                begin, rows = chunk(lane, phase, 0)
                into, shift = (g, 0) if phase == "rs1" else (outs[lane], xh * lane_rows(lane) - bases[lane])
                add(into, shift, begin, [TABLE[which][1] for which in ends], rows)
        if count == len(ORDER) * 3 // 5:
            inputs_sum()

    for i in (0, 1):
        across(i, 1).wait_send()
        across(i, -1).wait_send()

        @pl.when(away)
        def _():
            beside(i).wait_send()
            onward(i, 1).wait_send()
            onward(i, -1).wait_send()
    for i in range(2 * NCH):
        swap_p(i).wait_send()
        swap_a(i).wait_send()

    give(0, 1 - f).wait_send()
    give(1, 0).wait_send()
    give(1, 1).wait_send()

    @pl.when(away)
    def _():
        give(0, f).wait_send()
    for copy in outgoing[-SENDING:]:
        copy.wait_send()


PARTS = 8


def pieces(column):
    found, first, end = [], column * HALF, (column + 1) * HALF
    for lane in range(len(LANES)):
        low = (UPTO[lane] - LANES[lane][3]) * TILE * PIECES
        begin, stop = max(first, low), min(end, low + lane_rows(lane))
        if begin < stop:
            found.append((lane, begin - low, begin - first, stop - begin))
    return found


def widen(gin_ref, *refs):
    sums = refs[:len(LANES)]
    gin_out, up_out, down_out, wide, sem, write = refs[len(LANES):]
    through = pltpu.make_async_copy(gin_ref, gin_out, sem)
    through.start()
    columns = 2 * ROWS // PARTS // HALF
    writes = []
    for i in range(PARTS):
        first = i * columns
        half, column = first // 16, first % 16
        for j in range(columns):
            for lane, row, there, rows in pieces(column + j):
                row += half * lane_rows(lane)
                wide[there:there + rows, (first + j) * 128:(first + j + 1) * 128] = (
                    sums[lane][row:row + rows, :].astype(F32))
        if column < 8:
            there = up_out.at[:, pl.ds(half * QUARTER + column * 128, columns * 128)]
        else:
            there = down_out.at[pl.ds(half * QUARTER, QUARTER), pl.ds((column - 8) * 128, columns * 128)]
        writes.append(pltpu.make_async_copy(wide.at[:, pl.ds(first * 128, columns * 128)], there, write.at[i]))
        writes[i].start()
    through.wait()
    for copy in writes:
        copy.wait()


def shards(inputs, cotangent, w_up, w_down):
    vmem, anywhere = pl.BlockSpec(memory_space=pltpu.VMEM), pl.BlockSpec(memory_space=pl.ANY)
    gin_shape = jax.ShapeDtypeStruct((TOK, HALF), BF16)
    dma = pltpu.SemaphoreType.DMA
    grad_inputs, *sums = pl.pallas_call(
        body,
        name="ffn_backward",
        out_shape=(gin_shape, *(jax.ShapeDtypeStruct((2 * lane_rows(lane), 128), BF16) for lane in range(len(LANES)))),
        in_specs=[anywhere] * 4,
        out_specs=(vmem,) * (1 + len(LANES)),
        scratch_shapes=[
            pltpu.VMEM((TOK, HALF), BF16), pltpu.VMEM((TOK, HALF), BF16),
            pltpu.VMEM((2 * GRP, HALF), BF16), pltpu.VMEM((2 * GRP, HALF), BF16),
            pltpu.VMEM((HALF, 2 * GRP), BF16), pltpu.VMEM((QUARTER, 2 * GRP), BF16),
            pltpu.VMEM((HALF, QUARTER), BF16), pltpu.VMEM((QUARTER, HALF), BF16),
            pltpu.VMEM((2 * NCH, GRP, CH), F32), pltpu.VMEM((2 * NCH, GRP, CH), F32),
            pltpu.VMEM((2 * NCH, GRP, CH), F32),
            pltpu.VMEM((2 * NCH, GRP, CH), BF16), pltpu.VMEM((2 * NCH, GRP, CH), BF16),
            pltpu.VMEM((2 * GRP, QUARTER), BF16), pltpu.VMEM((2 * GRP, QUARTER), BF16),
            pltpu.VMEM((ROWS, 128), BF16), pltpu.VMEM((LANDING, 128), BF16),
            pltpu.VMEM((2 * GRP, HALF), BF16), pltpu.VMEM((4, TOK, HALF), BF16),
            dma((4,)), dma((2, 3)), dma((2, 4)), dma((2, 2)), dma((4 * NCH,)), dma((4 * NCH,)),
            dma((2, 2)), dma((4,)), dma((SENDING,)), dma((RECEIVING,)),
        ],
        compiler_params=pltpu.CompilerParams(
            collective_id=0, has_side_effects=True, vmem_limit_bytes=45 * 2**20),
    )(inputs, cotangent, w_up, w_down)
    return pl.pallas_call(
        widen,
        name="widen",
        out_shape=(gin_shape, jax.ShapeDtypeStruct((HALF, HID), F32), jax.ShapeDtypeStruct((HID, HALF), F32)),
        in_specs=[vmem] * (1 + len(LANES)),
        out_specs=(anywhere,) * 3,
        scratch_shapes=[
            pltpu.VMEM((HALF, 2 * HID), F32), dma, dma((PARTS,)),
        ],
        compiler_params=pltpu.CompilerParams(vmem_limit_bytes=26 * 2**20),
    )(grad_inputs, *sums)


def solution(mesh):
    return jax.shard_map(
        shards,
        mesh=mesh,
        in_specs=(P(("rep", "fs"), "tp"), P(("rep", "fs"), "tp"), P("fs", "tp"), P("tp", "fs")),
        out_specs=(P(("rep", "fs"), "tp"), P("fs", "tp"), P("tp", "fs")),
        check_vma=False,
    )
```

```python
import functools
import heapq

import jax
import jax.numpy as jnp
from jax import lax
from jax.experimental import pallas as pl
from jax.experimental.pallas import tpu as pltpu
from jax.sharding import PartitionSpec as P

MESH = pl.DeviceIdType.MESH
F32, BF16 = jnp.float32, jnp.bfloat16
NZ, NY, NX = 8, 4, 2
RINGS = {"y": NY, "z": NZ}
TOK, HALF, HID = 128, 1024, 2048
QUARTER = HID // 2
GRP = 2 * TOK
CH = 512
NCH = QUARTER // CH
ROWS = 2 * HALF * QUARTER // 128
TILE = 16
A, B = ("y", "z"), ("z", "y")
LANES = (
    (*B, -1, 2, True), (*B, 1, 2, True), (*A, -1, 2, False), (*B, -1, 2, False),
    (*A, 1, 2, True), (*A, 1, 2, False), (*B, 1, 2, False), (*B, 1, 2, False),
    (*B, -1, 2, False), (*A, 1, 2, False), (*B, 1, 2, False), (*A, 1, 2, True),
    (*A, -1, 2, False), (*A, -1, 2, False), (*A, 1, 2, True), (*A, -1, 2, True),
)
UPTO = tuple(sum(lane[3] for lane in LANES[:i + 1]) for i in range(len(LANES)))
STARTS = tuple(2.4 * tiles / 32 for tiles in UPTO)
PIECES = NY * NZ
RATE, LAG, WINDOW, WORK = 46000.0, 2.0, 1.2, 0.12
XFREE = 20.0
RANKS = {
    "rs1": (15, 121, 3, 111, 7, 93, 115, 43, 98, 65, 127, 92, 23, 49, 55, 12),
    "rs2": (71, 8, 37, 95, 125, 78, 85, 126, 0, 76, 17, 107, 84, 68, 32, 29),
    "x": (91, 73, 57, 74, 39, 24, 105, 103, 34, 81, 62, 59, 83, 75, 53, 42),
    "ag2": (99, 72, 101, 94, 88, 64, 100, 56, 30, 20, 120, 67, 16, 11, 33, 45),
    "ag1": (19, 96, 90, 119, 1, 52, 28, 108, 87, 38, 110, 35, 89, 9, 50, 10),
    "far2": (4, 69, 82, 77, 80, 46, 66, 70, 116, 60, 31, 5, 2, 14, 51, 102),
    "far1": (40, 124, 97, 113, 117, 41, 109, 27, 112, 122, 79, 47, 118, 21, 44, 54),
    "xl": (114, 106, 86, 25, 18, 61, 26, 104, 63, 6, 22, 123, 36, 13, 58, 48),
}
FIRST = ("rs1", "ag1", "far1", "xl")
SENDING = 24


def hops(n, arm):
    return n // 2 if arm == 0 else n // 2 - 1


def ring_of(lane, phase):
    return LANES[lane][0 if phase in FIRST else 1]


def length(lane, phase):
    piece = LANES[lane][3] * TILE
    return piece * RINGS[LANES[lane][1]] if phase in FIRST else piece


def lane_rows(lane):
    return LANES[lane][3] * TILE * PIECES


def last(lane, phase, arm, k):
    return phase == "x" or k == hops(RINGS[ring_of(lane, phase)], arm)


def way_of(lane, phase, arm):
    if phase in ("x", "xl"):
        return "x", 0
    way = LANES[lane][2] if arm == 0 else -LANES[lane][2]
    return ring_of(lane, phase), -way if phase[:2] == "rs" else way


def arrivals(lane, phase):
    n = RINGS[ring_of(lane, phase)]
    if phase == "x":
        return [(lane, phase, 0, 1)]
    if phase == "xl":
        return [(lane, phase, 0, 0)] + [(lane, phase, arm, k) for arm in (0, 1) for k in range(1, hops(n, arm) + 1)]
    if phase == "ag1" and LANES[lane][4]:
        return []
    return [(lane, phase, arm, hops(n, arm)) for arm in (0, 1)]


def planned():
    order, free, ready, flying, joined, now, count = [], {"x": XFREE}, {}, [], {}, 0.0, 0

    def want(lane, phase, arm, k):
        nonlocal count
        count += 1
        line = ready.setdefault(way_of(lane, phase, arm), [])
        heapq.heappush(line, (RANKS[phase][lane], -k, count, (lane, phase, arm, k)))

    def begin(lane, phase):
        joined[lane, phase] = 0
        for arm in (0,) if phase == "x" else (0, 1):
            want(lane, phase, arm, 1)

    def clear(link):
        return free.get("x" if link[0] == "x" else link, 0.0)

    def issue():
        nonlocal count
        for link, line in ready.items():
            while line and max(now, clear(link)) - now < WINDOW:
                what = heapq.heappop(line)[3]
                done = max(now, clear(link)) + length(what[0], what[1]) * 256 / RATE
                free["x" if link[0] == "x" else link] = done
                count += 1
                heapq.heappush(flying, (done + LAG, count, what))
                order.append(("send",) + what)

    todo = sorted((at, lane) for lane, at in enumerate(STARTS))
    while todo or flying:
        if todo and (not flying or todo[0][0] <= flying[0][0]):
            at, lane = todo.pop(0)
            now = max(now, at)
            order.append(("begin", lane))
            begin(lane, "rs1")
        else:
            at, _, (lane, phase, arm, k) = heapq.heappop(flying)
            now = max(now, at)
            late = LANES[lane][4]
            if phase == "xl":
                joined[lane, phase] += 1
                if joined[lane, phase] == RINGS[LANES[lane][0]]:
                    order.append(("end", lane, phase))
                    now += WORK
            elif late and phase == "ag1":
                now += WORK
                order.append(("pass", lane, phase, arm, k))
                if not last(lane, phase, arm, k):
                    want(lane, phase, arm, k + 1)
                else:
                    joined[lane, phase] += 1
                    if joined[lane, phase] == 2:
                        order.append(("end", lane, phase))
                want(lane, "xl", arm, k)
            elif not last(lane, phase, arm, k):
                now += WORK
                order.append(("pass", lane, phase, arm, k))
                want(lane, phase, arm, k + 1)
            else:
                joined[lane, phase] += 1
                if phase == "x" or joined[lane, phase] == 2:
                    now += WORK
                    order.append(("end", lane, phase))
                    for after in {"rs1": ("rs2",), "rs2": ("ag2",) if late else ("x", "ag2"), "x": ("far2",),
                                  "ag2": ("ag1",), "far2": ("far1",)}.get(phase, ()):
                        begin(lane, after)
                    if late and phase == "ag2":
                        joined[lane, "xl"] = 0
                        want(lane, "xl", 0, 0)
        issue()
        if not flying and not todo and any(ready.values()):
            now = min(clear(link) for link, line in ready.items() if line)
            issue()
    return order, now


ORDER, ESTIMATE = planned()


def transfers():
    sent, waited = {}, {}
    for at, step in enumerate(ORDER):
        if step[0] == "send":
            sent[step[1:]] = at
        elif step[0] == "pass":
            waited[step[1:]] = at
        elif step[0] == "end":
            waited.update((what, at) for what in arrivals(*step[1:]))
    table, rows, slots, back = {}, 0, [], {}
    for what in sent:
        back.setdefault(way_of(*what[:3]), []).append((sent[what], waited[what]))
    for what in sorted(sent, key=sent.get):
        ring, way = way_of(*what[:3])
        chosen = None
        for i, (link, free) in enumerate(slots):
            if link == (ring, way) and free < sent[what]:
                chosen = i
                break
        if chosen is None:
            chosen = len(slots)
            slots.append(None)
        heard = [end for begin, end in back[ring, -way] if begin > waited[what]]
        slots[chosen] = (ring, way), min(heard, default=len(ORDER))
        lands = what[1][:2] == "rs"
        table[what] = (chosen, rows if lands else None)
        rows += length(what[0], what[1]) if lands else 0
    return table, rows, len(slots)


TABLE, LANDING, RECEIVING = transfers()


def dot(a, b, dims):
    return lax.dot_general(a, b, (dims, ((), ())), preferred_element_type=F32)


def body(in_ref, cot_ref, up_ref, down_ref, gin_ref, *refs):
    outs = refs[:len(LANES)]
    (in_v, cot_v, x, c, xt, sqt, up, down, p_own, p_far, a_own, a_out, a_far, pre, sq, g, land, r, r_in,
     local_sem, xs, xr, fsem, ds, dr, gs, gr, ss, rs) = refs[len(LANES):]
    rep, f, t = lax.axis_index("rep"), lax.axis_index("fs"), lax.axis_index("tp")
    xh = lax.rem(rep, NX)
    yz = rep // NX
    xpos = xh * 2 + t
    pos = {"y": lax.rem(yz, NY), "z": yz // NY}

    def at(ring, step):
        n = RINGS[ring]
        there = dict(pos)
        there[ring] = lax.rem(pos[ring] + step + n, n)
        return ((there["z"] * NY + there["y"]) * NX + xh, f, t)

    def along(step, who):
        there = lax.rem(xpos + step + 4, 4)
        return (yz * NX + there // 2, who, lax.rem(there, 2))

    core = (rep, 1 - f, t)
    xpeer = (yz * NX + 1 - xh, f, t)
    home = f == t
    away = jnp.logical_not(home)

    share = pl.ds(pl.multiple_of(xh * QUARTER, QUARTER), QUARTER)
    w_copies = [pltpu.make_async_copy(up_ref.at[:, share], up, local_sem.at[0]),
                pltpu.make_async_copy(down_ref.at[share, :], down, local_sem.at[1])]
    t_copies = [pltpu.make_async_copy(in_ref, in_v, local_sem.at[2]),
                pltpu.make_async_copy(cot_ref, cot_v, local_sem.at[3])]
    for copy in t_copies + w_copies:
        copy.start()

    barrier = pltpu.get_barrier_semaphore()
    partners = [core] + [along(step, who) for step in (1, -1, 2) for who in (0, 1)] + [
        at("y", 1), at("y", -1), at("z", 1), at("z", -1)]
    for who in partners:
        pl.semaphore_signal(barrier, inc=1, device_id=who, device_id_type=MESH)
    pl.semaphore_wait(barrier, len(partners))

    def remote(src, dst, send, recv, who):
        return pltpu.make_async_remote_copy(
            src_ref=src, dst_ref=dst, send_sem=send, recv_sem=recv, device_id=who, device_id_type=MESH)

    def block(group, who):
        return pl.ds(pl.multiple_of((group * 2 + who) * TOK, TOK), TOK)

    pairs = ((in_v, x), (cot_v, c))

    def across(i, way):
        src, dst = pairs[i]
        group = t if way == 1 else 1 - t
        return remote(src, dst.at[block(group, f)], xs.at[i, 0 if way == 1 else 1],
                      xr.at[i, group * 2 + f], along(way, t))

    def beside(i):
        src, dst = pairs[i]
        return remote(src, dst.at[block(0, f)], xs.at[i, 2], xr.at[i, f], core)

    def onward(i, way):
        _, dst = pairs[i]
        group, who = (1 - t, 0) if way == 1 else (t, 1)
        return remote(dst.at[block(group, who)], dst.at[block(1, who)], fsem.at[i, who],
                      xr.at[i, 2 + who], along(way, f))

    def landed(i, group, who):
        _, dst = pairs[i]
        there = dst.at[block(group, who)]
        remote(there, there, xs.at[i, 0], xr.at[i, group * 2 + who], core).wait_recv()

    for i in (0, 1):
        t_copies[i].wait()
        across(i, 1).start()
        across(i, -1).start()
        src, dst = pairs[i]

        @pl.when(home)
        def _():
            dst[block(0, f), :] = src[...]

        @pl.when(away)
        def _():
            beside(i).start()

    def pass_on(i):
        @pl.when(away)
        def _():
            landed(i, 1 - t, 0)
            onward(i, 1).start()
            landed(i, t, 1)
            onward(i, -1).start()

    def arrive(i, group):
        if group == 0:
            @pl.when(home)
            def _():
                landed(i, 0, 1 - f)
        else:
            @pl.when(home)
            def _():
                landed(i, 1, 0)
                landed(i, 1, 1)

        @pl.when(away)
        def _():
            landed(i, group, jnp.where(group == t, 0, 1))

    def swap_p(i):
        return remote(p_own.at[i], p_far.at[i], ds.at[i], dr.at[i], core)

    def swap_a(i):
        return remote(a_out.at[i], a_far.at[i], ds.at[2 * NCH + i], dr.at[2 * NCH + i], core)

    def first_product(group):
        arrive(0, group)
        here = pl.ds(group * GRP, GRP)
        for j in range(NCH):
            i = group * NCH + j
            p_own[i] = dot(x[here, :], up[:, j * CH:(j + 1) * CH], ((1,), (0,)))
            swap_p(i).start()
        xt[:, here] = x[here, :].T

    def second_product(group):
        arrive(1, group)
        here = pl.ds(group * GRP, GRP)
        for j in range(NCH):
            i = group * NCH + j
            part = dot(c[here, :], down[j * CH:(j + 1) * CH, :], ((1,), (1,)))
            a_own[i] = part
            a_out[i] = part.astype(BF16)
            swap_a(i).start()

    pass_on(0)
    for w in w_copies:
        w.wait()
    first_product(0)
    pass_on(1)
    second_product(0)
    first_product(1)
    second_product(1)

    def activations(j):
        cols = slice(j * CH, (j + 1) * CH)
        for group in (0, 1):
            i = group * NCH + j
            swap_p(i).wait_recv()
            swap_a(i).wait_recv()
            here = slice(group * GRP, (group + 1) * GRP)
            relu = jnp.maximum(p_own[i] + p_far[i], 0.0)
            sq[here, cols] = (relu * relu).astype(BF16)
            grad = a_own[i] + a_far[i].astype(F32)
            pre[here, cols] = (2.0 * relu * grad).astype(BF16)

    def local_up(j):
        activations(j)
        part = dot(xt[...], pre[:, j * CH:(j + 1) * CH], ((1,), (0,)))
        for k in range(CH // 128):
            g[(j * 4 + k) * HALF:(j * 4 + k + 1) * HALF, :] = part[:, k * 128:(k + 1) * 128].astype(BF16)

    def local_down(j):
        if j == 0:
            sqt[...] = sq[...].T
        part = dot(sqt[...], c[:, j * CH:(j + 1) * CH], ((1,), (0,)))
        for k in range(CH // 128):
            g[(8 + j * 4 + k) * HALF:(9 + j * 4 + k) * HALF, :] = part[:, k * 128:(k + 1) * 128].astype(BF16)

    def inputs_part(j):
        rows = slice(j * 256, (j + 1) * 256)
        r[:, rows] = dot(pre[...], up[rows, :], ((1,), (1,))).astype(BF16)

    def give(group, who):
        there = jnp.where(group == 0, xh, 1 - xh)
        return remote(r.at[block(group, who)], r_in.at[xpos], gs.at[group, who], gr.at[xpos],
                      (yz * NX + there, who, f))

    def give_all():
        @pl.when(home)
        def _():
            give(0, 1 - f).start()
            r_in[xpos] = r[block(0, f), :]

        @pl.when(away)
        def _():
            give(0, f).start()
            give(0, 1 - f).start()

        give(1, 0).start()
        give(1, 1).start()

    def inputs_sum():
        def came(k):
            there = r_in.at[k]
            remote(there, there, gs.at[0, 0], gr.at[k], core).wait_recv()

        @pl.when(away)
        def _():
            came(xpos)

        for step in (1, 2, 3):
            came(lax.rem(xpos + step, 4))
        total = r_in[0].astype(F32)
        for k in range(1, 4):
            total += r_in[k].astype(F32)
        gin_ref[...] = total.astype(BF16)

    bases, base = [], 0
    for lane in range(len(LANES)):
        bases.append(base)
        base += LANES[lane][3] * TILE * PIECES
    started, outgoing = {}, []

    def chunk(lane, phase, step):
        ring = ring_of(lane, phase)
        rows = length(lane, phase)
        if phase[:2] == "rs":
            start = bases[lane]
        elif phase[:3] == "far":
            start = (1 - xh) * lane_rows(lane)
        else:
            start = xh * lane_rows(lane)
        if phase not in FIRST:
            start += pos[LANES[lane][0]] * length(lane, "rs1")
        n = RINGS[ring]
        there = lax.rem(pos[ring] + LANES[lane][2] * step + n, n)
        return pl.multiple_of(start + there * rows, TILE), rows

    def send(lane, phase, arm, k):
        index, slot = TABLE[lane, phase, arm, k]
        ring = ring_of(lane, phase)
        way = LANES[lane][2] if arm == 0 else -LANES[lane][2]
        if phase == "x":
            begin, rows = chunk(lane, phase, 0)
            src = dst = outs[lane].at[pl.ds(begin, rows)]
            who = xpeer
        elif phase == "xl":
            begin, rows = chunk(lane, phase, -k if arm == 0 else k)
            src = dst = outs[lane].at[pl.ds(begin, rows)]
            who = xpeer
        elif slot is not None:
            left = hops(RINGS[ring], arm) - k + 1
            begin, rows = chunk(lane, phase, -left if arm == 0 else left)
            src, dst, who = g.at[pl.ds(begin, rows)], land.at[pl.ds(slot, rows)], at(ring, -way)
        else:
            begin, rows = chunk(lane, phase, 1 - k if arm == 0 else k - 1)
            src = dst = outs[lane].at[pl.ds(begin, rows)]
            who = at(ring, way)
        if len(outgoing) >= SENDING:
            outgoing[-SENDING].wait_send()
        copy = remote(src, dst, ss.at[len(outgoing) % SENDING], rs.at[index], who)
        copy.start()
        outgoing.append(copy)
        started[lane, phase, arm, k] = copy

    def add(target, shift, begin, slots, rows):
        unit = max(u for u in range(TILE, 193, TILE) if rows % u == 0)

        @pl.loop(0, rows // unit)
        def _(i):
            here = pl.multiple_of(begin + i * unit, TILE)
            total = g[pl.ds(here, unit), :].astype(F32)
            for slot in slots:
                total += land[pl.ds(pl.multiple_of(slot + i * unit, TILE), unit), :].astype(F32)
            target[pl.ds(pl.multiple_of(here + shift, TILE), unit), :] = total.astype(BF16)

    aside = [functools.partial(inputs_part, j) for j in range(4)] + [give_all]
    begun = chunks = 0
    for count, step in enumerate(ORDER):
        kind, lane = step[:2]
        if kind == "begin":
            begun += 1
            while chunks * 8 < UPTO[lane]:
                (local_up, local_down)[chunks // 2](chunks % 2)
                chunks += 1
        elif kind == "send":
            send(*step[1:])
        elif kind == "pass":
            phase, arm, k = step[2:]
            started[lane, phase, arm, k].wait_recv()
            if phase[:2] == "rs":
                left = hops(RINGS[ring_of(lane, phase)], arm) - k
                begin, rows = chunk(lane, phase, -left if arm == 0 else left)
                add(g, 0, begin, (TABLE[lane, phase, arm, k][1],), rows)
            if begun == len(LANES) and aside:
                aside.pop(0)()
        else:
            phase = step[2]
            ends = arrivals(lane, phase)
            for which in ends:
                started[which].wait_recv()
            if phase[:2] == "rs":
                begin, rows = chunk(lane, phase, 0)
                into, shift = (g, 0) if phase == "rs1" else (outs[lane], xh * lane_rows(lane) - bases[lane])
                add(into, shift, begin, [TABLE[which][1] for which in ends], rows)
        if count == len(ORDER) * 3 // 5:
            inputs_sum()

    for i in (0, 1):
        across(i, 1).wait_send()
        across(i, -1).wait_send()

        @pl.when(away)
        def _():
            beside(i).wait_send()
            onward(i, 1).wait_send()
            onward(i, -1).wait_send()
    for i in range(2 * NCH):
        swap_p(i).wait_send()
        swap_a(i).wait_send()

    give(0, 1 - f).wait_send()
    give(1, 0).wait_send()
    give(1, 1).wait_send()

    @pl.when(away)
    def _():
        give(0, f).wait_send()
    for copy in outgoing[-SENDING:]:
        copy.wait_send()


PARTS = 8


def pieces(column):
    found, first, end = [], column * HALF, (column + 1) * HALF
    for lane in range(len(LANES)):
        low = (UPTO[lane] - LANES[lane][3]) * TILE * PIECES
        begin, stop = max(first, low), min(end, low + lane_rows(lane))
        if begin < stop:
            found.append((lane, begin - low, begin - first, stop - begin))
    return found


def widen(gin_ref, *refs):
    sums = refs[:len(LANES)]
    gin_out, up_out, down_out, wide, sem, write = refs[len(LANES):]
    through = pltpu.make_async_copy(gin_ref, gin_out, sem)
    through.start()
    columns = 2 * ROWS // PARTS // HALF
    writes = []
    for i in range(PARTS):
        first = i * columns
        half, column = first // 16, first % 16
        for j in range(columns):
            for lane, row, there, rows in pieces(column + j):
                row += half * lane_rows(lane)
                wide[there:there + rows, (first + j) * 128:(first + j + 1) * 128] = (
                    sums[lane][row:row + rows, :].astype(F32))
        if column < 8:
            there = up_out.at[:, pl.ds(half * QUARTER + column * 128, columns * 128)]
        else:
            there = down_out.at[pl.ds(half * QUARTER, QUARTER), pl.ds((column - 8) * 128, columns * 128)]
        writes.append(pltpu.make_async_copy(wide.at[:, pl.ds(first * 128, columns * 128)], there, write.at[i]))
        writes[i].start()
    through.wait()
    for copy in writes:
        copy.wait()


def shards(inputs, cotangent, w_up, w_down):
    vmem, anywhere = pl.BlockSpec(memory_space=pltpu.VMEM), pl.BlockSpec(memory_space=pl.ANY)
    gin_shape = jax.ShapeDtypeStruct((TOK, HALF), BF16)
    dma = pltpu.SemaphoreType.DMA
    grad_inputs, *sums = pl.pallas_call(
        body,
        name="ffn_backward",
        out_shape=(gin_shape, *(jax.ShapeDtypeStruct((2 * lane_rows(lane), 128), BF16) for lane in range(len(LANES)))),
        in_specs=[anywhere] * 4,
        out_specs=(vmem,) * (1 + len(LANES)),
        scratch_shapes=[
            pltpu.VMEM((TOK, HALF), BF16), pltpu.VMEM((TOK, HALF), BF16),
            pltpu.VMEM((2 * GRP, HALF), BF16), pltpu.VMEM((2 * GRP, HALF), BF16),
            pltpu.VMEM((HALF, 2 * GRP), BF16), pltpu.VMEM((QUARTER, 2 * GRP), BF16),
            pltpu.VMEM((HALF, QUARTER), BF16), pltpu.VMEM((QUARTER, HALF), BF16),
            pltpu.VMEM((2 * NCH, GRP, CH), F32), pltpu.VMEM((2 * NCH, GRP, CH), F32),
            pltpu.VMEM((2 * NCH, GRP, CH), F32),
            pltpu.VMEM((2 * NCH, GRP, CH), BF16), pltpu.VMEM((2 * NCH, GRP, CH), BF16),
            pltpu.VMEM((2 * GRP, QUARTER), BF16), pltpu.VMEM((2 * GRP, QUARTER), BF16),
            pltpu.VMEM((ROWS, 128), BF16), pltpu.VMEM((LANDING, 128), BF16),
            pltpu.VMEM((2 * GRP, HALF), BF16), pltpu.VMEM((4, TOK, HALF), BF16),
            dma((4,)), dma((2, 3)), dma((2, 4)), dma((2, 2)), dma((4 * NCH,)), dma((4 * NCH,)),
            dma((2, 2)), dma((4,)), dma((SENDING,)), dma((RECEIVING,)),
        ],
        compiler_params=pltpu.CompilerParams(
            collective_id=0, has_side_effects=True, vmem_limit_bytes=45 * 2**20),
    )(pltpu.with_memory_space_constraint(inputs, pltpu.HBM), pltpu.with_memory_space_constraint(cotangent, pltpu.HBM), w_up, w_down)
    return pl.pallas_call(
        widen,
        name="widen",
        out_shape=(gin_shape, jax.ShapeDtypeStruct((HALF, HID), F32), jax.ShapeDtypeStruct((HID, HALF), F32)),
        in_specs=[vmem] * (1 + len(LANES)),
        out_specs=(anywhere,) * 3,
        scratch_shapes=[
            pltpu.VMEM((HALF, 2 * HID), F32), dma, dma((PARTS,)),
        ],
        compiler_params=pltpu.CompilerParams(vmem_limit_bytes=26 * 2**20),
    )(grad_inputs, *sums)


def solution(mesh):
    return jax.shard_map(
        shards,
        mesh=mesh,
        in_specs=(P(("rep", "fs"), "tp"), P(("rep", "fs"), "tp"), P("fs", "tp"), P("tp", "fs")),
        out_specs=(P(("rep", "fs"), "tp"), P("fs", "tp"), P("tp", "fs")),
        check_vma=False,
    )
```

```python
import functools
import heapq

import jax
import jax.numpy as jnp
from jax import lax
from jax.experimental import pallas as pl
from jax.experimental.pallas import tpu as pltpu
from jax.sharding import PartitionSpec as P

MESH = pl.DeviceIdType.MESH
F32, BF16 = jnp.float32, jnp.bfloat16
NZ, NY, NX = 8, 4, 2
RINGS = {"y": NY, "z": NZ}
TOK, HALF, HID = 128, 1024, 2048
QUARTER = HID // 2
GRP = 2 * TOK
CH = 512
NCH = QUARTER // CH
ROWS = 2 * HALF * QUARTER // 128
TILE = 16
A, B = ("y", "z"), ("z", "y")
LANES = (
    (*B, -1, 2, True), (*B, 1, 2, True), (*A, -1, 2, False), (*B, -1, 2, False),
    (*A, 1, 2, True), (*A, 1, 2, False), (*B, 1, 2, False), (*B, 1, 2, False),
    (*B, -1, 2, False), (*A, 1, 2, False), (*B, 1, 2, False), (*A, 1, 2, True),
    (*A, -1, 2, False), (*A, -1, 2, False), (*A, 1, 2, True), (*A, -1, 2, True),
)
UPTO = tuple(sum(lane[3] for lane in LANES[:i + 1]) for i in range(len(LANES)))
STARTS = tuple(2.4 * tiles / 32 for tiles in UPTO)
PIECES = NY * NZ
RATE, LAG, WINDOW, WORK = 46000.0, 2.0, 1.2, 0.12
XFREE = 20.0
RANKS = {
    "rs1": (15, 121, 3, 111, 7, 93, 115, 43, 98, 65, 127, 92, 23, 49, 55, 12),
    "rs2": (71, 8, 37, 95, 125, 78, 85, 126, 0, 76, 17, 107, 84, 68, 32, 29),
    "x": (91, 73, 57, 74, 39, 24, 105, 103, 34, 81, 62, 59, 83, 75, 53, 42),
    "ag2": (99, 72, 101, 94, 88, 64, 100, 56, 30, 20, 120, 67, 16, 11, 33, 45),
    "ag1": (19, 96, 90, 119, 1, 52, 28, 108, 87, 38, 110, 35, 89, 9, 50, 10),
    "far2": (4, 69, 82, 77, 80, 46, 66, 70, 116, 60, 31, 5, 2, 14, 51, 102),
    "far1": (40, 124, 97, 113, 117, 41, 109, 27, 112, 122, 79, 47, 118, 21, 44, 54),
    "xl": (114, 106, 86, 25, 18, 61, 26, 104, 63, 6, 22, 123, 36, 13, 58, 48),
}
FIRST = ("rs1", "ag1", "far1", "xl")
SENDING = 24


def hops(n, arm):
    return n // 2 if arm == 0 else n // 2 - 1


def ring_of(lane, phase):
    return LANES[lane][0 if phase in FIRST else 1]


def length(lane, phase):
    piece = LANES[lane][3] * TILE
    return piece * RINGS[LANES[lane][1]] if phase in FIRST else piece


def lane_rows(lane):
    return LANES[lane][3] * TILE * PIECES


def last(lane, phase, arm, k):
    return phase == "x" or k == hops(RINGS[ring_of(lane, phase)], arm)


def way_of(lane, phase, arm):
    if phase in ("x", "xl"):
        return "x", 0
    way = LANES[lane][2] if arm == 0 else -LANES[lane][2]
    return ring_of(lane, phase), -way if phase[:2] == "rs" else way


def arrivals(lane, phase):
    n = RINGS[ring_of(lane, phase)]
    if phase == "x":
        return [(lane, phase, 0, 1)]
    if phase == "xl":
        return [(lane, phase, 0, 0)] + [(lane, phase, arm, k) for arm in (0, 1) for k in range(1, hops(n, arm) + 1)]
    if phase == "ag1" and LANES[lane][4]:
        return []
    return [(lane, phase, arm, hops(n, arm)) for arm in (0, 1)]


def planned():
    order, free, ready, flying, joined, now, count = [], {"x": XFREE}, {}, [], {}, 0.0, 0

    def want(lane, phase, arm, k):
        nonlocal count
        count += 1
        line = ready.setdefault(way_of(lane, phase, arm), [])
        heapq.heappush(line, (RANKS[phase][lane], -k, count, (lane, phase, arm, k)))

    def begin(lane, phase):
        joined[lane, phase] = 0
        for arm in (0,) if phase == "x" else (0, 1):
            want(lane, phase, arm, 1)

    def clear(link):
        return free.get("x" if link[0] == "x" else link, 0.0)

    def issue():
        nonlocal count
        for link, line in ready.items():
            while line and max(now, clear(link)) - now < WINDOW:
                what = heapq.heappop(line)[3]
                done = max(now, clear(link)) + length(what[0], what[1]) * 256 / RATE
                free["x" if link[0] == "x" else link] = done
                count += 1
                heapq.heappush(flying, (done + LAG, count, what))
                order.append(("send",) + what)

    todo = sorted((at, lane) for lane, at in enumerate(STARTS))
    while todo or flying:
        if todo and (not flying or todo[0][0] <= flying[0][0]):
            at, lane = todo.pop(0)
            now = max(now, at)
            order.append(("begin", lane))
            begin(lane, "rs1")
        else:
            at, _, (lane, phase, arm, k) = heapq.heappop(flying)
            now = max(now, at)
            late = LANES[lane][4]
            if phase == "xl":
                joined[lane, phase] += 1
                if joined[lane, phase] == RINGS[LANES[lane][0]]:
                    order.append(("end", lane, phase))
                    now += WORK
            elif late and phase == "ag1":
                now += WORK
                order.append(("pass", lane, phase, arm, k))
                if not last(lane, phase, arm, k):
                    want(lane, phase, arm, k + 1)
                else:
                    joined[lane, phase] += 1
                    if joined[lane, phase] == 2:
                        order.append(("end", lane, phase))
                want(lane, "xl", arm, k)
            elif not last(lane, phase, arm, k):
                now += WORK
                order.append(("pass", lane, phase, arm, k))
                want(lane, phase, arm, k + 1)
            else:
                joined[lane, phase] += 1
                if phase == "x" or joined[lane, phase] == 2:
                    now += WORK
                    order.append(("end", lane, phase))
                    for after in {"rs1": ("rs2",), "rs2": ("ag2",) if late else ("x", "ag2"), "x": ("far2",),
                                  "ag2": ("ag1",), "far2": ("far1",)}.get(phase, ()):
                        begin(lane, after)
                    if late and phase == "ag2":
                        joined[lane, "xl"] = 0
                        want(lane, "xl", 0, 0)
        issue()
        if not flying and not todo and any(ready.values()):
            now = min(clear(link) for link, line in ready.items() if line)
            issue()
    return order, now


ORDER, ESTIMATE = planned()


def transfers():
    sent, waited = {}, {}
    for at, step in enumerate(ORDER):
        if step[0] == "send":
            sent[step[1:]] = at
        elif step[0] == "pass":
            waited[step[1:]] = at
        elif step[0] == "end":
            waited.update((what, at) for what in arrivals(*step[1:]))
    table, rows, slots, back = {}, 0, [], {}
    for what in sent:
        back.setdefault(way_of(*what[:3]), []).append((sent[what], waited[what]))
    for what in sorted(sent, key=sent.get):
        ring, way = way_of(*what[:3])
        chosen = None
        for i, (link, free) in enumerate(slots):
            if link == (ring, way) and free < sent[what]:
                chosen = i
                break
        if chosen is None:
            chosen = len(slots)
            slots.append(None)
        heard = [end for begin, end in back[ring, -way] if begin > waited[what]]
        slots[chosen] = (ring, way), min(heard, default=len(ORDER))
        lands = what[1][:2] == "rs"
        table[what] = (chosen, rows if lands else None)
        rows += length(what[0], what[1]) if lands else 0
    return table, rows, len(slots)


TABLE, LANDING, RECEIVING = transfers()


def dot(a, b, dims):
    return lax.dot_general(a, b, (dims, ((), ())), preferred_element_type=F32)


def body(in_ref, cot_ref, up_ref, down_ref, gin_ref, *refs):
    outs = refs[:len(LANES)]
    (in_v, cot_v, x, c, xt, sqt, up, down, p_own, p_far, a_own, a_out, a_far, pre, sq, g, land, r, r_in,
     local_sem, xs, xr, fsem, ds, dr, gs, gr, ss, rs) = refs[len(LANES):]
    rep, f, t = lax.axis_index("rep"), lax.axis_index("fs"), lax.axis_index("tp")
    xh = lax.rem(rep, NX)
    yz = rep // NX
    xpos = xh * 2 + t
    pos = {"y": lax.rem(yz, NY), "z": yz // NY}

    def at(ring, step):
        n = RINGS[ring]
        there = dict(pos)
        there[ring] = lax.rem(pos[ring] + step + n, n)
        return ((there["z"] * NY + there["y"]) * NX + xh, f, t)

    def along(step, who):
        there = lax.rem(xpos + step + 4, 4)
        return (yz * NX + there // 2, who, lax.rem(there, 2))

    core = (rep, 1 - f, t)
    xpeer = (yz * NX + 1 - xh, f, t)
    home = f == t
    away = jnp.logical_not(home)

    share = pl.ds(pl.multiple_of(xh * QUARTER, QUARTER), QUARTER)
    w_copies = [pltpu.make_async_copy(up_ref.at[:, share], up, local_sem.at[0]),
                pltpu.make_async_copy(down_ref.at[share, :], down, local_sem.at[1])]
    t_copies = [pltpu.make_async_copy(in_ref, in_v, local_sem.at[2]),
                pltpu.make_async_copy(cot_ref, cot_v, local_sem.at[3])]
    for copy in t_copies + w_copies:
        copy.start()

    barrier = pltpu.get_barrier_semaphore()
    partners = [core] + [along(step, who) for step in (1, -1, 2) for who in (0, 1)] + [
        at("y", 1), at("y", -1), at("z", 1), at("z", -1)]
    for who in partners:
        pl.semaphore_signal(barrier, inc=1, device_id=who, device_id_type=MESH)
    pl.semaphore_wait(barrier, len(partners))

    def remote(src, dst, send, recv, who):
        return pltpu.make_async_remote_copy(
            src_ref=src, dst_ref=dst, send_sem=send, recv_sem=recv, device_id=who, device_id_type=MESH)

    def block(group, who):
        return pl.ds(pl.multiple_of((group * 2 + who) * TOK, TOK), TOK)

    pairs = ((in_v, x), (cot_v, c))

    def across(i, way):
        src, dst = pairs[i]
        group = t if way == 1 else 1 - t
        return remote(src, dst.at[block(group, f)], xs.at[i, 0 if way == 1 else 1],
                      xr.at[i, group * 2 + f], along(way, t))

    def beside(i):
        src, dst = pairs[i]
        return remote(src, dst.at[block(0, f)], xs.at[i, 2], xr.at[i, f], core)

    def onward(i, way):
        _, dst = pairs[i]
        group, who = (1 - t, 0) if way == 1 else (t, 1)
        return remote(dst.at[block(group, who)], dst.at[block(1, who)], fsem.at[i, who],
                      xr.at[i, 2 + who], along(way, f))

    def landed(i, group, who):
        _, dst = pairs[i]
        there = dst.at[block(group, who)]
        remote(there, there, xs.at[i, 0], xr.at[i, group * 2 + who], core).wait_recv()

    for i in (0, 1):
        t_copies[i].wait()
        across(i, 1).start()
        across(i, -1).start()
        src, dst = pairs[i]

        @pl.when(home)
        def _():
            dst[block(0, f), :] = src[...]

        @pl.when(away)
        def _():
            beside(i).start()

    def pass_on(i):
        @pl.when(away)
        def _():
            landed(i, 1 - t, 0)
            onward(i, 1).start()
            landed(i, t, 1)
            onward(i, -1).start()

    def arrive(i, group):
        if group == 0:
            @pl.when(home)
            def _():
                landed(i, 0, 1 - f)
        else:
            @pl.when(home)
            def _():
                landed(i, 1, 0)
                landed(i, 1, 1)

        @pl.when(away)
        def _():
            landed(i, group, jnp.where(group == t, 0, 1))

    def swap_p(i):
        return remote(p_own.at[i], p_far.at[i], ds.at[i], dr.at[i], core)

    def swap_a(i):
        return remote(a_out.at[i], a_far.at[i], ds.at[2 * NCH + i], dr.at[2 * NCH + i], core)

    def first_product(group):
        arrive(0, group)
        here = pl.ds(group * GRP, GRP)
        for j in range(NCH):
            i = group * NCH + j
            p_own[i] = dot(x[here, :], up[:, j * CH:(j + 1) * CH], ((1,), (0,)))
            swap_p(i).start()
        xt[:, here] = x[here, :].T

    def second_product(group):
        arrive(1, group)
        here = pl.ds(group * GRP, GRP)
        for j in range(NCH):
            i = group * NCH + j
            part = dot(c[here, :], down[j * CH:(j + 1) * CH, :], ((1,), (1,)))
            a_own[i] = part
            a_out[i] = part.astype(BF16)
            swap_a(i).start()

    pass_on(0)
    for w in w_copies:
        w.wait()
    first_product(0)
    pass_on(1)
    second_product(0)
    first_product(1)
    second_product(1)

    def activations(j):
        cols = slice(j * CH, (j + 1) * CH)
        for group in (0, 1):
            i = group * NCH + j
            swap_p(i).wait_recv()
            swap_a(i).wait_recv()
            here = slice(group * GRP, (group + 1) * GRP)
            relu = jnp.maximum(p_own[i] + p_far[i], 0.0)
            sq[here, cols] = (relu * relu).astype(BF16)
            grad = a_own[i] + a_far[i].astype(F32)
            pre[here, cols] = (2.0 * relu * grad).astype(BF16)

    def local_up(j):
        activations(j)
        part = dot(xt[...], pre[:, j * CH:(j + 1) * CH], ((1,), (0,)))
        for k in range(CH // 128):
            g[(j * 4 + k) * HALF:(j * 4 + k + 1) * HALF, :] = part[:, k * 128:(k + 1) * 128].astype(BF16)

    def local_down(j):
        if j == 0:
            sqt[...] = sq[...].T
        part = dot(sqt[...], c[:, j * CH:(j + 1) * CH], ((1,), (0,)))
        for k in range(CH // 128):
            g[(8 + j * 4 + k) * HALF:(9 + j * 4 + k) * HALF, :] = part[:, k * 128:(k + 1) * 128].astype(BF16)

    def inputs_part(j):
        rows = slice(j * 256, (j + 1) * 256)
        r[:, rows] = dot(pre[...], up[rows, :], ((1,), (1,))).astype(BF16)

    def give(group, who):
        there = jnp.where(group == 0, xh, 1 - xh)
        return remote(r.at[block(group, who)], r_in.at[xpos], gs.at[group, who], gr.at[xpos],
                      (yz * NX + there, who, f))

    def give_all():
        @pl.when(home)
        def _():
            give(0, 1 - f).start()
            r_in[xpos] = r[block(0, f), :]

        @pl.when(away)
        def _():
            give(0, f).start()
            give(0, 1 - f).start()

        give(1, 0).start()
        give(1, 1).start()

    def inputs_sum():
        def came(k):
            there = r_in.at[k]
            remote(there, there, gs.at[0, 0], gr.at[k], core).wait_recv()

        @pl.when(away)
        def _():
            came(xpos)

        for step in (1, 2, 3):
            came(lax.rem(xpos + step, 4))
        total = r_in[0].astype(F32)
        for k in range(1, 4):
            total += r_in[k].astype(F32)
        gin_ref[...] = total.astype(BF16)

    bases, base = [], 0
    for lane in range(len(LANES)):
        bases.append(base)
        base += LANES[lane][3] * TILE * PIECES
    started, outgoing = {}, []

    def chunk(lane, phase, step):
        ring = ring_of(lane, phase)
        rows = length(lane, phase)
        if phase[:2] == "rs":
            start = bases[lane]
        elif phase[:3] == "far":
            start = (1 - xh) * lane_rows(lane)
        else:
            start = xh * lane_rows(lane)
        if phase not in FIRST:
            start += pos[LANES[lane][0]] * length(lane, "rs1")
        n = RINGS[ring]
        there = lax.rem(pos[ring] + LANES[lane][2] * step + n, n)
        return pl.multiple_of(start + there * rows, TILE), rows

    def send(lane, phase, arm, k):
        index, slot = TABLE[lane, phase, arm, k]
        ring = ring_of(lane, phase)
        way = LANES[lane][2] if arm == 0 else -LANES[lane][2]
        if phase == "x":
            begin, rows = chunk(lane, phase, 0)
            src = dst = outs[lane].at[pl.ds(begin, rows)]
            who = xpeer
        elif phase == "xl":
            begin, rows = chunk(lane, phase, -k if arm == 0 else k)
            src = dst = outs[lane].at[pl.ds(begin, rows)]
            who = xpeer
        elif slot is not None:
            left = hops(RINGS[ring], arm) - k + 1
            begin, rows = chunk(lane, phase, -left if arm == 0 else left)
            src, dst, who = g.at[pl.ds(begin, rows)], land.at[pl.ds(slot, rows)], at(ring, -way)
        else:
            begin, rows = chunk(lane, phase, 1 - k if arm == 0 else k - 1)
            src = dst = outs[lane].at[pl.ds(begin, rows)]
            who = at(ring, way)
        if len(outgoing) >= SENDING:
            outgoing[-SENDING].wait_send()
        copy = remote(src, dst, ss.at[len(outgoing) % SENDING], rs.at[index], who)
        copy.start()
        outgoing.append(copy)
        started[lane, phase, arm, k] = copy

    def add(target, shift, begin, slots, rows):
        unit = max(u for u in range(TILE, 193, TILE) if rows % u == 0)

        @pl.loop(0, rows // unit)
        def _(i):
            here = pl.multiple_of(begin + i * unit, TILE)
            total = g[pl.ds(here, unit), :].astype(F32)
            for slot in slots:
                total += land[pl.ds(pl.multiple_of(slot + i * unit, TILE), unit), :].astype(F32)
            target[pl.ds(pl.multiple_of(here + shift, TILE), unit), :] = total.astype(BF16)

    aside = [functools.partial(inputs_part, j) for j in range(4)] + [give_all]
    begun = chunks = 0
    for count, step in enumerate(ORDER):
        kind, lane = step[:2]
        if kind == "begin":
            begun += 1
            while chunks * 8 < UPTO[lane]:
                (local_up, local_down)[chunks // 2](chunks % 2)
                chunks += 1
        elif kind == "send":
            send(*step[1:])
        elif kind == "pass":
            phase, arm, k = step[2:]
            started[lane, phase, arm, k].wait_recv()
            if phase[:2] == "rs":
                left = hops(RINGS[ring_of(lane, phase)], arm) - k
                begin, rows = chunk(lane, phase, -left if arm == 0 else left)
                add(g, 0, begin, (TABLE[lane, phase, arm, k][1],), rows)
            if begun == len(LANES) and aside and count % 3 == 0:
                aside.pop(0)()
        else:
            phase = step[2]
            ends = arrivals(lane, phase)
            for which in ends:
                started[which].wait_recv()
            if phase[:2] == "rs":
                begin, rows = chunk(lane, phase, 0)
                into, shift = (g, 0) if phase == "rs1" else (outs[lane], xh * lane_rows(lane) - bases[lane])
                add(into, shift, begin, [TABLE[which][1] for which in ends], rows)
        if count == len(ORDER) * 3 // 5:
            inputs_sum()

    for i in (0, 1):
        across(i, 1).wait_send()
        across(i, -1).wait_send()

        @pl.when(away)
        def _():
            beside(i).wait_send()
            onward(i, 1).wait_send()
            onward(i, -1).wait_send()
    for i in range(2 * NCH):
        swap_p(i).wait_send()
        swap_a(i).wait_send()

    give(0, 1 - f).wait_send()
    give(1, 0).wait_send()
    give(1, 1).wait_send()

    @pl.when(away)
    def _():
        give(0, f).wait_send()
    for copy in outgoing[-SENDING:]:
        copy.wait_send()


PARTS = 8


def pieces(column):
    found, first, end = [], column * HALF, (column + 1) * HALF
    for lane in range(len(LANES)):
        low = (UPTO[lane] - LANES[lane][3]) * TILE * PIECES
        begin, stop = max(first, low), min(end, low + lane_rows(lane))
        if begin < stop:
            found.append((lane, begin - low, begin - first, stop - begin))
    return found


def widen(gin_ref, *refs):
    sums = refs[:len(LANES)]
    gin_out, up_out, down_out, wide, sem, write = refs[len(LANES):]
    through = pltpu.make_async_copy(gin_ref, gin_out, sem)
    through.start()
    columns = 2 * ROWS // PARTS // HALF
    writes = []
    for i in range(PARTS):
        first = i * columns
        half, column = first // 16, first % 16
        for j in range(columns):
            for lane, row, there, rows in pieces(column + j):
                row += half * lane_rows(lane)
                wide[there:there + rows, (first + j) * 128:(first + j + 1) * 128] = (
                    sums[lane][row:row + rows, :].astype(F32))
        if column < 8:
            there = up_out.at[:, pl.ds(half * QUARTER + column * 128, columns * 128)]
        else:
            there = down_out.at[pl.ds(half * QUARTER, QUARTER), pl.ds((column - 8) * 128, columns * 128)]
        writes.append(pltpu.make_async_copy(wide.at[:, pl.ds(first * 128, columns * 128)], there, write.at[i]))
        writes[i].start()
    through.wait()
    for copy in writes:
        copy.wait()


def shards(inputs, cotangent, w_up, w_down):
    vmem, anywhere = pl.BlockSpec(memory_space=pltpu.VMEM), pl.BlockSpec(memory_space=pl.ANY)
    gin_shape = jax.ShapeDtypeStruct((TOK, HALF), BF16)
    dma = pltpu.SemaphoreType.DMA
    grad_inputs, *sums = pl.pallas_call(
        body,
        name="ffn_backward",
        out_shape=(gin_shape, *(jax.ShapeDtypeStruct((2 * lane_rows(lane), 128), BF16) for lane in range(len(LANES)))),
        in_specs=[anywhere] * 4,
        out_specs=(vmem,) * (1 + len(LANES)),
        scratch_shapes=[
            pltpu.VMEM((TOK, HALF), BF16), pltpu.VMEM((TOK, HALF), BF16),
            pltpu.VMEM((2 * GRP, HALF), BF16), pltpu.VMEM((2 * GRP, HALF), BF16),
            pltpu.VMEM((HALF, 2 * GRP), BF16), pltpu.VMEM((QUARTER, 2 * GRP), BF16),
            pltpu.VMEM((HALF, QUARTER), BF16), pltpu.VMEM((QUARTER, HALF), BF16),
            pltpu.VMEM((2 * NCH, GRP, CH), F32), pltpu.VMEM((2 * NCH, GRP, CH), F32),
            pltpu.VMEM((2 * NCH, GRP, CH), F32),
            pltpu.VMEM((2 * NCH, GRP, CH), BF16), pltpu.VMEM((2 * NCH, GRP, CH), BF16),
            pltpu.VMEM((2 * GRP, QUARTER), BF16), pltpu.VMEM((2 * GRP, QUARTER), BF16),
            pltpu.VMEM((ROWS, 128), BF16), pltpu.VMEM((LANDING, 128), BF16),
            pltpu.VMEM((2 * GRP, HALF), BF16), pltpu.VMEM((4, TOK, HALF), BF16),
            dma((4,)), dma((2, 3)), dma((2, 4)), dma((2, 2)), dma((4 * NCH,)), dma((4 * NCH,)),
            dma((2, 2)), dma((4,)), dma((SENDING,)), dma((RECEIVING,)),
        ],
        compiler_params=pltpu.CompilerParams(
            collective_id=0, has_side_effects=True, vmem_limit_bytes=45 * 2**20),
    )(pltpu.with_memory_space_constraint(inputs, pltpu.HBM), pltpu.with_memory_space_constraint(cotangent, pltpu.HBM), w_up, w_down)
    return pl.pallas_call(
        widen,
        name="widen",
        out_shape=(gin_shape, jax.ShapeDtypeStruct((HALF, HID), F32), jax.ShapeDtypeStruct((HID, HALF), F32)),
        in_specs=[vmem] * (1 + len(LANES)),
        out_specs=(anywhere,) * 3,
        scratch_shapes=[
            pltpu.VMEM((HALF, 2 * HID), F32), dma, dma((PARTS,)),
        ],
        compiler_params=pltpu.CompilerParams(vmem_limit_bytes=26 * 2**20),
    )(grad_inputs, *sums)


def solution(mesh):
    return jax.shard_map(
        shards,
        mesh=mesh,
        in_specs=(P(("rep", "fs"), "tp"), P(("rep", "fs"), "tp"), P("fs", "tp"), P("tp", "fs")),
        out_specs=(P(("rep", "fs"), "tp"), P("fs", "tp"), P("tp", "fs")),
        check_vma=False,
    )
```
